32 devices in a mesh: grp: 2 (over y), fs: 4 (over z), tp: 4 (over x, core).
Axes of the slice: x: 2, y: 2, z: 4, core: 2. Of those that a mesh axis runs over, the one named last changes fastest.
Arguments:
- tokens: bfloat16 [6144, 2048], P(('grp', 'fs'), 'tp'), parts along dimension 0, may hold values from -6 to 6
- recurrent_norm_gain: float32 [2048], replicated, may hold values from 0.1 to 1.9
- channel_norm_gain: float32 [2048], replicated, may hold values from 0.1 to 1.9
- gate_projection_weight: float32 [2048, 2048], P('fs', 'tp'), may hold values from -0.125 to 0.125
- gate_column_scale: float32 [2048], P(('tp', 'fs')), may hold values from 0.5 to 2
- input_projection_weight: float32 [2048, 2048], P('fs', 'tp'), may hold values from -0.125 to 0.125
- input_column_scale: float32 [2048], P(('tp', 'fs')), may hold values from 0.5 to 2
- convolution_kernel: float32 [4, 2048], P(None, 'tp'), may hold values from -3 to 3
- recurrence_gate_weight: float32 [8, 256, 256], P('tp', 'fs'), may hold values from -0.375 to 0.375
- recurrence_column_scale: float32 [8, 256], P('tp', 'fs'), may hold values from 0.25 to 4
- input_gate_weight: float32 [8, 256, 256], P('tp', 'fs'), may hold values from -0.375 to 0.375
- input_gate_column_scale: float32 [8, 256], P('tp', 'fs'), may hold values from 0.5 to 2
- channel_decay_param: float32 [2048], P('tp'), may hold values from 2.2 to 8.5
- position_decay_shift: float32 [6144], P(('grp', 'fs')), parts along dimension 0, may hold values from -0.7 to 0
- output_projection_weight: float32 [2048, 2048], P('tp', 'fs'), may hold values from -0.125 to 0.125
- output_column_scale: float32 [2048], P('fs'), may hold values from 0.5 to 2
- mixer_gate_weight: float32 [2048, 5632], P('fs', 'tp'), may hold values from -0.125 to 0.125
- mixer_gate_column_scale: float32 [5632], P(('tp', 'fs')), may hold values from 0.5 to 2
- up_projection_weight: float32 [2048, 5632], P('fs', 'tp'), may hold values from -0.125 to 0.125
- up_column_scale: float32 [5632], P(('tp', 'fs')), may hold values from 0.5 to 2
- down_projection_weight: float32 [5632, 2048], P('tp', 'fs'), may hold values from -0.078125 to 0.078125
- down_column_scale: float32 [2048], P('fs'), may hold values from 0.5 to 2
Outputs:
- layer_out: bfloat16 [6144, 2048], P(('grp', 'fs'), 'tp'), parts along dimension 0
The draws below stay inside these ranges and needn't reach their ends.
There are 2 independent parts, one for each index of `grp`. The reference program is written for one: setup_inputs(seed, part) draws one part's arguments, and reference() takes and returns one part's arrays. A program takes and returns all parts, laid end to end along the dimension named above; an argument that names none is the same for every part. Nothing has to cross between parts.
All inputs are finite; a program needn't handle non-finite values.
Results may differ from the reference program's by a relative error of at most 0.023.
Values may be sent and summed in bfloat16 or wider, within the bound.
A program may use at most 128 MiB of HBM per device.

```python
import math
import jax
import jax.numpy as jnp
from jax import lax

D = 2048
LRU = 2048
BW = 256
FF = 5632
TAPS = 4
SEQ_LEN = 128
BLOCKS = 8
TOKENS = 3072
N_TP = 4


def draw_channel_decay_param(key, part):
    pick_key, slow_key, fast_key = jax.random.split(jax.random.fold_in(key, 11), 3)
    fast_share = 0.5
    is_fast = jax.random.uniform(pick_key, (LRU,), jnp.float32) < fast_share
    slow_rate = jnp.exp(jax.random.uniform(slow_key, (LRU,), jnp.float32, jnp.log(0.05 / SEQ_LEN), jnp.log(0.3 / SEQ_LEN)))
    fast_rate = jnp.exp(jax.random.uniform(fast_key, (LRU,), jnp.float32, jnp.log(0.03), jnp.log(0.1)))
    rate = jnp.where(is_fast, fast_rate, slow_rate)
    return -jnp.log(jnp.expm1(rate))


def draw_position_decay_shift(key, part):
    place_key, depth_key = jax.random.split(jax.random.fold_in(key, 23))
    seq_count = TOKENS // SEQ_LEN
    places = jax.random.randint(place_key, (seq_count, 1, 4), 1, SEQ_LEN)
    within = jnp.arange(SEQ_LEN)[None, :, None]
    struck = jnp.any(within == places, axis=2)
    depth = jax.random.uniform(depth_key, (seq_count, SEQ_LEN), jnp.float32, jnp.log(0.5), jnp.log(0.8))
    return jnp.where(struck, depth, 0.0).reshape(TOKENS)


def level_of(stream_key, dims, pieces, low, top_value):
    gain, own = 1.0, jax.random.fold_in(stream_key, 6)
    for dim, parts in pieces:
        draws = jnp.exp(jax.random.uniform(jax.random.fold_in(own, dim), (parts,), jnp.float32, low / len(pieces), top_value / len(pieces)))
        gain = gain * jnp.repeat(draws, dims[dim] // parts).reshape([-1 if axis == dim else 1 for axis in range(len(dims))])
    return gain


def centred(stream_key, extent, width, bound, cuts=(), dtype=jnp.bfloat16):
    array = width * jax.random.normal(stream_key, extent, jnp.float32)
    if cuts:
        array = array * level_of(stream_key, extent, cuts, -0.22, 0.18)
    return jnp.clip(array, -bound, bound).astype(dtype)


def setup_inputs(seed: int = 0, part: int = 0) -> dict:
    arg_keys = jax.random.split(jax.random.key(seed), 23)
    own_keys = jax.random.split(jax.random.fold_in(arg_keys[22], part), 23)
    tokens = centred(own_keys[0], (TOKENS, D), 1.0, 6.0, ((0, 4), (1, 4)))
    recurrent_norm_gain = jnp.clip(1.0 + 0.18 * jax.random.normal(arg_keys[1], (D,), jnp.float32), 0.1, 1.9)
    channel_norm_gain = jnp.clip(1.0 + 0.18 * jax.random.normal(arg_keys[2], (D,), jnp.float32), 0.1, 1.9)
    gate_projection_weight = centred(arg_keys[3], (D, LRU), D ** -0.5, 0.125, ((0, 4), (1, 4)), jnp.float32)
    gate_column_scale = jnp.clip(jnp.exp(math.log(2.0) - 1.3862944 * jax.random.uniform(arg_keys[4], (LRU,), jnp.float32) ** level_of(arg_keys[4], (LRU,), ((0, 16),), -0.2, 0.2)), 0.5, 2.0)
    input_projection_weight = centred(arg_keys[5], (D, LRU), D ** -0.5, 0.125, ((0, 4), (1, 4)), jnp.float32)
    input_column_scale = jnp.clip(jnp.exp(math.log(2.0) - 1.3862944 * jax.random.uniform(arg_keys[6], (LRU,), jnp.float32) ** level_of(arg_keys[6], (LRU,), ((0, 16),), -0.2, 0.2)), 0.5, 2.0)
    convolution_kernel = centred(arg_keys[7], (TAPS, LRU), 0.5, 3.0, ((1, 4),), jnp.float32)
    recurrence_gate_weight = centred(arg_keys[8], (BLOCKS, BW, BW), BW ** -0.5, 0.375, ((0, 4), (1, 4)), jnp.float32)
    recurrence_column_scale = jnp.clip(jnp.exp(math.log(4.0) - 2.7725887 * jax.random.uniform(arg_keys[9], (BLOCKS, BW), jnp.float32) ** level_of(arg_keys[9], (BLOCKS, BW), ((0, 4), (1, 4)), -0.2, 0.2)), 0.25, 4.0)
    input_gate_weight = centred(arg_keys[10], (BLOCKS, BW, BW), BW ** -0.5, 0.375, ((0, 4), (1, 4)), jnp.float32)
    input_gate_column_scale = jnp.clip(jnp.exp(math.log(2.0) - 1.3862944 * jax.random.uniform(arg_keys[11], (BLOCKS, BW), jnp.float32) ** level_of(arg_keys[11], (BLOCKS, BW), ((0, 4), (1, 4)), -0.2, 0.2)), 0.5, 2.0)
    channel_decay_param = draw_channel_decay_param(jax.random.fold_in(arg_keys[22], 71), part)
    position_decay_shift = draw_position_decay_shift(jax.random.fold_in(jax.random.fold_in(arg_keys[22], part), 71), part)
    output_projection_weight = centred(arg_keys[14], (LRU, D), LRU ** -0.5, 0.125, ((0, 4), (1, 4)), jnp.float32)
    output_column_scale = jnp.clip(jnp.exp(math.log(2.0) - 1.3862944 * jax.random.uniform(arg_keys[15], (D,), jnp.float32) ** level_of(arg_keys[15], (D,), ((0, 4),), -0.2, 0.2)), 0.5, 2.0)
    mixer_gate_weight = centred(arg_keys[16], (D, FF), D ** -0.5, 0.125, ((0, 4), (1, 4)), jnp.float32)
    mixer_gate_column_scale = jnp.clip(jnp.exp(math.log(2.0) - 1.3862944 * jax.random.uniform(arg_keys[17], (FF,), jnp.float32) ** level_of(arg_keys[17], (FF,), ((0, 16),), -0.2, 0.2)), 0.5, 2.0)
    up_projection_weight = centred(arg_keys[18], (D, FF), D ** -0.5, 0.125, ((0, 4), (1, 4)), jnp.float32)
    up_column_scale = jnp.clip(jnp.exp(math.log(2.0) - 1.3862944 * jax.random.uniform(arg_keys[19], (FF,), jnp.float32) ** level_of(arg_keys[19], (FF,), ((0, 16),), -0.2, 0.2)), 0.5, 2.0)
    down_projection_weight = centred(arg_keys[20], (FF, D), FF ** -0.5, 0.078125, ((0, 4), (1, 4)), jnp.float32)
    down_column_scale = jnp.clip(jnp.exp(math.log(2.0) - 1.3862944 * jax.random.uniform(arg_keys[21], (D,), jnp.float32) ** level_of(arg_keys[21], (D,), ((0, 4),), -0.2, 0.2)), 0.5, 2.0)
    return {"tokens": tokens, "recurrent_norm_gain": recurrent_norm_gain, "channel_norm_gain": channel_norm_gain, "gate_projection_weight": gate_projection_weight, "gate_column_scale": gate_column_scale, "input_projection_weight": input_projection_weight, "input_column_scale": input_column_scale, "convolution_kernel": convolution_kernel, "recurrence_gate_weight": recurrence_gate_weight, "recurrence_column_scale": recurrence_column_scale, "input_gate_weight": input_gate_weight, "input_gate_column_scale": input_gate_column_scale, "channel_decay_param": channel_decay_param, "position_decay_shift": position_decay_shift, "output_projection_weight": output_projection_weight, "output_column_scale": output_column_scale, "mixer_gate_weight": mixer_gate_weight, "mixer_gate_column_scale": mixer_gate_column_scale, "up_projection_weight": up_projection_weight, "up_column_scale": up_column_scale, "down_projection_weight": down_projection_weight, "down_column_scale": down_column_scale}


eps = 1e-06

def rms_rows(row_block, gain_vec):
    widened = row_block.astype(jnp.float32)
    scaled = widened * lax.rsqrt(lax.optimization_barrier(jnp.mean(widened * widened, axis=-1, keepdims=True)) + eps)
    return (scaled * gain_vec).astype(jnp.bfloat16)

def project(row_block, weight, column_scale):
    return jnp.dot(row_block, weight.astype(jnp.bfloat16), preferred_element_type=jnp.float32) * column_scale

def grouped_sum(row_block, weight, column_scale):
    group_width = row_block.shape[1] // N_TP
    summed = jnp.zeros((row_block.shape[0], weight.shape[1]), jnp.float32)
    for member in range(N_TP):
        first_col = member * group_width
        partial_term = project(row_block[:, first_col:first_col + group_width], weight[first_col:first_col + group_width], column_scale)
        summed = summed + lax.optimization_barrier(partial_term.astype(jnp.bfloat16)).astype(jnp.float32)
    return summed

def convolve(branch, convolution_kernel):
    row_count, channels = branch.shape
    framed = branch.astype(jnp.float32).reshape(row_count // SEQ_LEN, SEQ_LEN, channels)
    padded = jnp.pad(framed, ((0, 0), (TAPS - 1, 0), (0, 0)))
    summed = jnp.zeros_like(framed)
    for offset in range(TAPS):
        summed = summed + padded[:, TAPS - 1 - offset:TAPS - 1 - offset + SEQ_LEN] * convolution_kernel[offset]
    return summed.reshape(row_count, channels).astype(jnp.bfloat16)

def block_gate(convolved_output, weight, column_scale):
    row_count = convolved_output.shape[0]
    framed = convolved_output.astype(jnp.float32).reshape(row_count, weight.shape[0], weight.shape[1])
    rounded = lax.optimization_barrier(weight.astype(jnp.bfloat16)).astype(jnp.float32)
    preact = jnp.einsum('tni,nio->tno', framed, rounded) * column_scale
    return jax.nn.sigmoid(preact).reshape(row_count, -1)

def carried_state(convolved_output, recurrence_gate_value, input_gate_value, channel_decay_param, position_decay_shift):
    row_count, channels = convolved_output.shape
    log_retention = -8.0 * recurrence_gate_value * jax.nn.softplus(-channel_decay_param) + position_decay_shift[:, None]
    starts = (jnp.arange(row_count) % SEQ_LEN == 0)[:, None]
    factor = jnp.where(starts, 1.0, jnp.sqrt(-jnp.expm1(2.0 * log_retention)))
    drive = convolved_output.astype(jnp.float32) * input_gate_value * factor
    framed_shape = (row_count // SEQ_LEN, SEQ_LEN, channels)

    def combine(earlier, later):
        return (earlier[0] * later[0], later[0] * earlier[1] + later[1])
    _, hidden_states = lax.associative_scan(combine, (jnp.exp(log_retention).reshape(framed_shape), drive.reshape(framed_shape)), axis=1)
    return hidden_states.reshape(row_count, channels)

def reference(tokens, recurrent_norm_gain, channel_norm_gain, gate_projection_weight, gate_column_scale, input_projection_weight, input_column_scale, convolution_kernel, recurrence_gate_weight, recurrence_column_scale, input_gate_weight, input_gate_column_scale, channel_decay_param, position_decay_shift, output_projection_weight, output_column_scale, mixer_gate_weight, mixer_gate_column_scale, up_projection_weight, up_column_scale, down_projection_weight, down_column_scale):
    normed = rms_rows(tokens, recurrent_norm_gain)
    gate_branch = project(normed, gate_projection_weight, gate_column_scale).astype(jnp.bfloat16)
    input_branch = project(normed, input_projection_weight, input_column_scale).astype(jnp.bfloat16)
    convolved_output = convolve(input_branch, convolution_kernel)
    recurrence_gate_value = block_gate(convolved_output, recurrence_gate_weight, recurrence_column_scale)
    input_gate_value = block_gate(convolved_output, input_gate_weight, input_gate_column_scale)
    hidden_states = carried_state(convolved_output, recurrence_gate_value, input_gate_value, channel_decay_param, position_decay_shift)
    mixer_rows = (jax.nn.gelu(gate_branch.astype(jnp.float32)) * hidden_states).astype(jnp.bfloat16)
    mixer_sum = grouped_sum(mixer_rows, output_projection_weight, output_column_scale)
    hidden = (tokens.astype(jnp.float32) + mixer_sum).astype(jnp.bfloat16)
    channel_normed = rms_rows(hidden, channel_norm_gain)
    swish_pre = project(channel_normed, mixer_gate_weight, mixer_gate_column_scale)
    upward_pre = project(channel_normed, up_projection_weight, up_column_scale)
    activation = (jax.nn.silu(swish_pre) * upward_pre).astype(jnp.bfloat16)
    channel_sum = grouped_sum(activation, down_projection_weight, down_column_scale)
    return (hidden.astype(jnp.float32) + channel_sum).astype(jnp.bfloat16)
```

```python
import jax
import jax.numpy as jnp
from jax import lax
from jax.experimental import pallas as pl
from jax.experimental.pallas import tpu as pltpu
from jax.sharding import PartitionSpec as P

TAPS = 4
SEQ_LEN = 128
LANES = 128
MESH = pl.DeviceIdType.MESH

eps = 1e-06


def shares(total, parts):
    parts = min(parts, total)
    return [total // parts + (1 if i < total % parts else 0) for i in range(parts)]


def ring_plan(costs, count, latency):
    ready = {(c, 0): 0.0 for c in range(len(costs))}
    free, plan, landed = 0.0, [], {}
    while ready:
        at_hand = [k for k in ready if ready[k] <= free]
        if not at_hand:
            free = min(ready.values())
            continue
        c, s = min(at_hand, key=lambda k: (k[0], -k[1]))
        begin = free
        del ready[(c, s)]
        free = free + costs[c]
        landed[(c, s)] = free + latency
        plan.append((begin, c, s))
        if s + 1 < count - 1:
            ready[(c, s + 1)] = free + latency
    for c in range(len(costs)):
        plan.append((landed[(c, count - 2)], c, count - 1))
    return sorted(plan), landed


def layer_body(dims, *refs):
    (n, copies, tp, rows, model, dc, rec, blocks, brows, width, hid, col) = dims
    (
        tokens, wpair, wblk, wout, wff, wdn, scales, gain1, gain2, taps, decay, shift, out,
        Wp, Wb, Wo, Wf, Wd, X, H, N, UG, M, T1, R1, T2, R2, A, S, SV,
        z_send, z_recv, y_send, y_recv, own_sem, tok_sem,
        x_send, x_recv, r1_send, r1_recv, h_send, h_recv, r2_send, r2_recv, s_send, s_recv,
    ) = refs
    g, f, t = lax.axis_index("grp"), lax.axis_index("fs"), lax.axis_index("tp")
    krows = model // n

    barrier = pltpu.get_barrier_semaphore()
    for axis, count, here in (("fs", n, f), ("grp", copies, g), ("tp", tp, t)):
        for k in range(1, count):
            pl.semaphore_signal(
                barrier, inc=1, device_id={axis: lax.rem(here + k, count)}, device_id_type=MESH
            )

    def remote(src, dst, send, recv, axis, index):
        return pltpu.make_async_remote_copy(
            src_ref=src, dst_ref=dst, send_sem=send, recv_sem=recv,
            device_id={axis: index}, device_id_type=MESH,
        )

    chunks, tags = [], {}

    def by_rows(buf, source, first, wide):
        per = krows // copies

        def view(owner, share):
            return buf.at[pl.ds(pl.multiple_of(owner * krows + share * per, per), per), pl.ds(first, wide)]

        return (
            view,
            source.at[:, pl.ds(first, wide)],
            lambda: buf.at[pl.ds(pl.multiple_of(f * krows, krows), krows), pl.ds(first, wide)],
            per * wide,
        )

    def by_columns(buf, source, first, wide):
        deep = buf.shape[0]
        per = deep // copies

        def view(owner, share):
            return buf.at[
                pl.ds(pl.multiple_of(share * per, per), per),
                pl.ds(pl.multiple_of(owner * col + first, LANES), wide),
            ]

        return (
            view,
            source.at[:, pl.ds(first, wide)],
            lambda: buf.at[:, pl.ds(pl.multiple_of(f * col + first, LANES), wide)],
            per * wide,
        )

    def by_blocks():
        per = 2 * width // copies

        def view(owner, share):
            return Wb.at[
                :, pl.ds(pl.multiple_of(owner * brows, brows), brows),
                pl.ds(pl.multiple_of(share * per, per), per),
            ]

        return (
            view,
            wblk,
            lambda: Wb.at[:, pl.ds(pl.multiple_of(f * brows, brows), brows), :],
            blocks * brows * per,
        )

    def add(tag, chunk):
        tags[tag] = len(chunks)
        chunks.append(chunk)

    add("in", by_rows(Wp, wpair, rec, rec))
    add("blk", by_blocks())
    add("gate", by_rows(Wp, wpair, 0, rec))
    add("out", by_columns(Wo, wout, 0, col))
    ff_groups, first = [], 0
    for pairs in shares(hid // LANES, 4):
        add(("ff", len(ff_groups)), by_rows(Wf, wff, first * 2 * LANES, pairs * 2 * LANES))
        ff_groups.append((first, pairs))
        first += pairs
    dn_groups, first = [], 0
    for lanes in shares(col // LANES, 3):
        add(("dn", len(dn_groups)), by_columns(Wd, wdn, first * LANES, lanes * LANES))
        dn_groups.append((first * LANES, lanes * LANES))
        first += lanes

    own = []
    for c, (view, source, place, cost) in enumerate(chunks):
        own.append(pltpu.make_async_copy(source, place(), own_sem.at[c]))
        own[c].start()
    tok = pltpu.make_async_copy(tokens, X.at[t], tok_sem.at[0])
    tok.start()
    S[f] = scales[...]

    pl.semaphore_wait(barrier, (n - 1) + (copies - 1) + (tp - 1))

    drains = []

    def send(copy):
        copy.start()
        drains.append(copy)

    def z_copy(c, s):
        owner = lax.rem(f - s + n, n)
        view = chunks[c][0](owner, g)
        return remote(view, view, z_send.at[c, s], z_recv.at[c, s], "fs", lax.rem(f + 1, n))

    def z_land(c, s):
        owner = lax.rem(f - s - 1 + n, n)
        view = chunks[c][0](owner, g)
        return remote(view, view, z_send.at[c, s], z_recv.at[c, s], "fs", lax.rem(f + 1, n))

    def y_copy(c, s, other, share):
        owner = lax.rem(f - s + n, n)
        view = chunks[c][0](owner, share)
        return remote(
            view, view, y_send.at[c, s - 1, other - 1], y_recv.at[c, s - 1, other - 1],
            "grp", lax.rem(g + other, copies),
        )

    def ring_step(c, s):
        if s == 0:
            own[c].wait()
        else:
            z_land(c, s - 1).wait_recv()
        if s < n - 1:
            send(z_copy(c, s))
        if s > 0:
            for other in range(1, copies):
                send(y_copy(c, s, other, g))

    def settled(c, s):
        for other in range(1, copies):
            y_copy(c, s, other, lax.rem(g - other + copies, copies)).wait_recv()

    def gathered(c):
        for s in range(1, n):
            settled(c, s)

    def spread(source, buf, sends, recvs):
        for k in range(1, tp):
            send(remote(source, buf.at[t], sends.at[k - 1], recvs.at[k - 1], "tp", lax.rem(t + k, tp)))

    def spread_land(buf, sends, recvs):
        for k in range(1, tp):
            place = buf.at[lax.rem(t - k + tp, tp)]
            remote(place, place, sends.at[k - 1], recvs.at[k - 1], "tp", lax.rem(t + k, tp)).wait_recv()

    spread(tokens, X, x_send, x_recv)
    for k in range(1, n):
        send(remote(scales, S.at[f], s_send.at[k - 1], s_recv.at[k - 1], "fs", lax.rem(f + k, n)))

    def norm(buf, gain):
        def tile(i, _):
            here = pl.ds(pl.multiple_of(i * SEQ_LEN, SEQ_LEN), SEQ_LEN)
            parts = [buf[p, here, :].astype(jnp.float32) for p in range(tp)]
            total = sum(jnp.sum(v * v, axis=-1, keepdims=True) for v in parts)
            factor = lax.rsqrt(total / model + eps)
            for p in range(tp):
                lanes = slice(p * dc, (p + 1) * dc)
                N[here, lanes] = (parts[p] * factor * gain[:, lanes]).astype(jnp.bfloat16)
            return 0

        lax.fori_loop(0, rows // SEQ_LEN, tile, 0)

    def first_norm():
        tok.wait()
        spread_land(X, x_send, x_recv)
        norm(X, gain1)

    def project(tag, first):
        def run():
            gathered(tags[tag])

            def tile(i, _):
                lanes = pl.ds(pl.multiple_of(first + i * 256, LANES), 256)
                summed = jnp.dot(N[...], Wp[:, lanes], preferred_element_type=jnp.float32)
                UG[:, lanes] = (summed * SV[:, lanes]).astype(jnp.bfloat16)
                return 0

            lax.fori_loop(0, rec // 256, tile, 0)

        return run

    def scale_sum():
        for k in range(1, n):
            place = S.at[lax.rem(f - k + n, n)]
            remote(place, place, s_send.at[k - 1], s_recv.at[k - 1], "fs", lax.rem(f + k, n)).wait_recv()
        total = S[0]
        for o in range(1, n):
            total = total + S[o]
        SV[...] = total

    def recurrence():
        gathered(tags["blk"])
        position = lax.broadcasted_iota(jnp.int32, (SEQ_LEN, width), 0)

        def sequence(i, _):
            here = pl.ds(pl.multiple_of(i * SEQ_LEN, SEQ_LEN), SEQ_LEN)
            moved_by = shift[here, :]
            for block in range(blocks):
                lanes = slice(block * width, (block + 1) * width)
                at = lambda base: slice(base + block * width, base + (block + 1) * width)
                branch = UG[here, at(rec)].astype(jnp.float32)
                summed = branch * taps[0:1, lanes]
                for offset in range(1, TAPS):
                    moved = jnp.where(position >= offset, pltpu.roll(branch, offset, 0), 0.0)
                    summed = summed + moved * taps[offset : offset + 1, lanes]
                conv = summed.astype(jnp.bfloat16)
                sums = jnp.dot(conv, Wb[block], preferred_element_type=jnp.float32)
                recur = jax.nn.sigmoid(sums[:, :width] * SV[:, at(2 * rec)])
                inject = jax.nn.sigmoid(sums[:, width:] * SV[:, at(3 * rec)])
                log_keep = -8.0 * recur * decay[:, lanes] + moved_by
                twice = 2.0 * log_keep
                near = -twice * (
                    1.0
                    + twice * (0.5 + twice * (1.0 / 6 + twice * (1.0 / 24 + twice * (1.0 / 120))))
                )
                lost = jnp.where(twice > -0.125, near, 1.0 - jnp.exp(twice))
                factor = jnp.where(position == 0, 1.0, jnp.sqrt(lost))
                state = conv.astype(jnp.float32) * inject * factor
                keep = jnp.exp(log_keep)
                reach = 1
                while reach < SEQ_LEN:
                    inside = position >= reach
                    state = state + keep * jnp.where(inside, pltpu.roll(state, reach, 0), 0.0)
                    keep = keep * jnp.where(inside, pltpu.roll(keep, reach, 0), 1.0)
                    reach *= 2
                gate = UG[here, lanes].astype(jnp.float32)
                M[here, lanes] = (jax.nn.gelu(gate) * state).astype(jnp.bfloat16)
            return 0

        lax.fori_loop(0, rows // SEQ_LEN, sequence, 0)

    def mix_out():
        gathered(tags["out"])
        for k in list(range(1, tp)) + [0]:
            peer = lax.rem(t + k, tp)
            lanes = pl.ds(pl.multiple_of(peer * dc, dc), dc)
            T1[k] = jnp.dot(M[...], Wo[:, lanes], preferred_element_type=jnp.float32).astype(jnp.bfloat16)
            if k:
                send(remote(T1.at[k], R1.at[k - 1], r1_send.at[k - 1], r1_recv.at[k - 1], "tp", peer))

    def hidden():
        for k in range(1, tp):
            place = R1.at[k - 1]
            remote(place, place, r1_send.at[k - 1], r1_recv.at[k - 1], "tp", lax.rem(t + k, tp)).wait_recv()

        def tile(i, _):
            here = pl.ds(pl.multiple_of(i * SEQ_LEN, SEQ_LEN), SEQ_LEN)
            total = T1[0, here, :].astype(jnp.float32)
            for k in range(1, tp):
                total = total + R1[k - 1, here, :].astype(jnp.float32)
            H[t, here, :] = (X[t, here, :].astype(jnp.float32) + total).astype(jnp.bfloat16)
            return 0

        lax.fori_loop(0, rows // SEQ_LEN, tile, 0)
        spread(H.at[t], H, h_send, h_recv)

    def second_norm():
        spread_land(H, h_send, h_recv)
        norm(H, gain2)

    def activate(index):
        first, pairs = ff_groups[index]

        def run():
            gathered(tags[("ff", index)])

            def tile(i, _):
                both = pl.ds(pl.multiple_of((first + i) * 2 * LANES, 2 * LANES), 2 * LANES)
                cols = pl.ds(pl.multiple_of(4 * rec + (first + i) * 2 * LANES, LANES), 2 * LANES)
                summed = jnp.dot(N[...], Wf[:, both], preferred_element_type=jnp.float32)
                summed = summed * SV[:, cols]
                one = pl.ds(pl.multiple_of((first + i) * LANES, LANES), LANES)
                A[:, one] = (jax.nn.silu(summed[:, :LANES]) * summed[:, LANES:]).astype(jnp.bfloat16)
                return 0

            lax.fori_loop(0, pairs, tile, 0)

        return run

    pieces = []

    def down(index, s):
        first, wide = dn_groups[index]

        def run():
            if s:
                settled(tags[("dn", index)], s)
            start = lax.rem(f - s + n, n) * col + first
            lanes = pl.ds(pl.multiple_of(start, LANES), wide)
            peer = start // dc
            inner = start - peer * dc
            T2[:, lanes] = jnp.dot(A[...], Wd[:, lanes], preferred_element_type=jnp.float32).astype(jnp.bfloat16)

            def piece():
                return remote(
                    T2.at[:, lanes], R2.at[t, :, pl.ds(pl.multiple_of(inner, LANES), wide)],
                    r2_send.at[index, s], r2_recv.at[t, inner // LANES], "tp", peer,
                )

            @pl.when(peer != t)
            def _():
                piece().start()

            pieces.append((peer, piece))

        return run

    def finish():
        for k in range(1, tp):
            peer = lax.rem(t + k, tp)
            for part in range(dc // col):
                for first, wide in dn_groups:
                    inner = part * col + first
                    place = R2.at[peer, :, pl.ds(inner, wide)]
                    remote(place, place, r2_send.at[0, 0], r2_recv.at[peer, inner // LANES], "tp", peer).wait_recv()

        def tile(i, _):
            here = pl.ds(pl.multiple_of(i * SEQ_LEN, SEQ_LEN), SEQ_LEN)
            total = T2[here, pl.ds(pl.multiple_of(t * dc, dc), dc)].astype(jnp.float32)
            for k in range(1, tp):
                total = total + R2[lax.rem(t + k, tp), here, :].astype(jnp.float32)
            out[here, :] = (H[t, here, :].astype(jnp.float32) + total).astype(jnp.bfloat16)
            return 0

        lax.fori_loop(0, rows // SEQ_LEN, tile, 0)

    link = 2 * 2 / 91e3
    costs = [chunk[3] * link for chunk in chunks]
    ring, landed = ring_plan(costs, n, 6.0)
    events = [(when, 0, c, s, None) for when, c, s in ring]

    def ready(tag, s=None):
        c = tags[tag]
        return landed[(c, (n if s is None else s + 1) - 2)] + costs[c] + 3.0

    clock = [0.0]

    def task(when, takes, run):
        clock[0] = max(clock[0], when)
        events.append((clock[0], 1, len(events), 0, run))
        clock[0] += takes

    across = tp * rows * dc * link / 1.0
    task(1.0, 0.5, scale_sum)
    task(across, 3.0, first_norm)
    task(ready("in"), 3.5, project("in", rec))
    task(ready("gate"), 3.5, project("gate", 0))
    task(ready("blk"), 7.0, recurrence)
    task(ready("out"), 4.0, mix_out)
    task(clock[0] + across, 2.0, hidden)
    task(clock[0] + across, 3.0, second_norm)
    for index in range(len(ff_groups)):
        task(ready(("ff", index)), 7.0, activate(index))
    for index in range(len(dn_groups)):
        for s in range(n):
            task(ready(("dn", index), s) if s else 0.0, 1.5, down(index, s))
    for _, kind, c, s, run in sorted(events, key=lambda e: e[:4]):
        if kind == 0:
            ring_step(c, s)
        else:
            run()
    finish()
    for copy in drains:
        copy.wait_send()
    for peer, piece in pieces:
        @pl.when(peer != t)
        def _(piece=piece):
            piece().wait_send()


def on_device(
    tokens,
    recurrent_norm_gain,
    channel_norm_gain,
    gate_projection_weight,
    gate_column_scale,
    input_projection_weight,
    input_column_scale,
    convolution_kernel,
    recurrence_gate_weight,
    recurrence_column_scale,
    input_gate_weight,
    input_gate_column_scale,
    channel_decay_param,
    position_decay_shift,
    output_projection_weight,
    output_column_scale,
    mixer_gate_weight,
    mixer_gate_column_scale,
    up_projection_weight,
    up_column_scale,
    down_projection_weight,
    down_column_scale,
):
    n, copies, tp = (lax.axis_size(axis) for axis in ("fs", "grp", "tp"))
    f = lax.axis_index("fs")
    narrow = lambda weight: weight.astype(jnp.bfloat16)
    rows, dc = tokens.shape
    model = dc * tp
    krows, rec = gate_projection_weight.shape
    blocks, brows, width = recurrence_gate_weight.shape
    ff = mixer_gate_weight.shape[1]
    hid = -(-ff // LANES) * LANES
    col = output_projection_weight.shape[1]

    def wide(scale):
        kept = scale.reshape(-1, 1, scale.shape[-1])
        owner = lax.broadcasted_iota(jnp.int32, (1, n, 1), 1)
        return jnp.where(owner == f, kept, 0.0).reshape(1, -1)

    def pairs(a, b):
        pad = ((0, 0), (0, hid - ff))
        a, b = (jnp.pad(v, pad).reshape(v.shape[0], -1, 1, LANES) for v in (a, b))
        return jnp.concatenate([a, b], axis=2).reshape(a.shape[0], -1)

    scales = jnp.concatenate(
        [
            wide(gate_column_scale),
            wide(input_column_scale),
            wide(recurrence_column_scale),
            wide(input_gate_column_scale),
            pairs(wide(mixer_gate_column_scale), wide(up_column_scale)),
        ],
        axis=1,
    )
    wpair = jnp.concatenate([narrow(gate_projection_weight), narrow(input_projection_weight)], axis=1)
    wblk = jnp.concatenate([narrow(recurrence_gate_weight), narrow(input_gate_weight)], axis=2)
    wout = narrow(output_projection_weight * output_column_scale)
    wff = pairs(narrow(mixer_gate_weight), narrow(up_projection_weight))
    wdn = jnp.pad(narrow(down_projection_weight * down_column_scale), ((0, hid - ff), (0, 0)))

    dims = (n, copies, tp, rows, model, dc, rec, blocks, brows, width, hid, col)
    chunk_count = 4 + len(shares(hid // LANES, 4)) + len(shares(col // LANES, 3))
    here = pl.BlockSpec(memory_space=pltpu.VMEM)
    away = pl.BlockSpec(memory_space=pl.ANY)
    bf = lambda *shape: pltpu.VMEM(shape, jnp.bfloat16)
    dma = lambda *shape: pltpu.SemaphoreType.DMA(shape)
    flops = 2 * rows * (model * (2 * rec + 2 * hid) + rec * 2 * width + rec * model + hid * model)
    return pl.pallas_call(
        lambda *refs: layer_body(dims, *refs),
        out_shape=jax.ShapeDtypeStruct((rows, dc), jnp.bfloat16),
        in_specs=[away] * 6 + [here] * 6,
        out_specs=here,
        scratch_shapes=[
            bf(model, 2 * rec),
            bf(blocks, n * brows, 2 * width),
            bf(rec, model),
            bf(model, 2 * hid),
            bf(hid, model),
            bf(tp, rows, dc),
            bf(tp, rows, dc),
            bf(rows, model),
            bf(rows, 2 * rec),
            bf(rows, rec),
            bf(tp, rows, dc),
            bf(tp - 1, rows, dc),
            bf(rows, model),
            bf(tp, rows, dc),
            bf(rows, hid),
            pltpu.VMEM((n,) + scales.shape, jnp.float32),
            pltpu.VMEM(scales.shape, jnp.float32),
            dma(chunk_count, n - 1),
            dma(chunk_count, n - 1),
            dma(chunk_count, n - 1, copies - 1),
            dma(chunk_count, n - 1, copies - 1),
            dma(chunk_count),
            dma(1),
            dma(tp - 1),
            dma(tp - 1),
            dma(tp - 1),
            dma(tp - 1),
            dma(tp - 1),
            dma(tp - 1),
            dma(len(shares(col // LANES, 3)), n),
            dma(tp, dc // LANES),
            dma(n - 1),
            dma(n - 1),
        ],
        compiler_params=pltpu.CompilerParams(
            collective_id=0, has_side_effects=True, vmem_limit_bytes=67_043_328
        ),
        cost_estimate=pl.CostEstimate(flops=flops, bytes_accessed=8 * rows * model, transcendentals=0),
    )(
        tokens,
        wpair,
        wblk,
        wout,
        wff,
        wdn,
        scales,
        recurrent_norm_gain[None, :],
        channel_norm_gain[None, :],
        convolution_kernel,
        jax.nn.softplus(-channel_decay_param)[None, :],
        position_decay_shift[:, None],
    )


def solution(mesh):
    placed = (
        P(("grp", "fs"), "tp"),
        P(),
        P(),
        P("fs", "tp"),
        P(("tp", "fs")),
        P("fs", "tp"),
        P(("tp", "fs")),
        P(None, "tp"),
        P("tp", "fs", None),
        P("tp", "fs"),
        P("tp", "fs", None),
        P("tp", "fs"),
        P("tp"),
        P(("grp", "fs")),
        P("tp", "fs"),
        P("fs"),
        P("fs", "tp"),
        P(("tp", "fs")),
        P("fs", "tp"),
        P(("tp", "fs")),
        P("tp", "fs"),
        P("fs"),
    )
    return jax.shard_map(
        on_device, mesh=mesh, in_specs=placed, out_specs=P(("grp", "fs"), "tp"), check_vma=False
    )
```

```python
import jax
import jax.numpy as jnp
from jax import lax
from jax.experimental import pallas as pl
from jax.experimental.pallas import tpu as pltpu
from jax.sharding import PartitionSpec as P

TAPS = 4
SEQ_LEN = 128
LANES = 128
TILE = 64
MESH = pl.DeviceIdType.MESH

eps = 1e-06


def shares(total, parts):
    parts = min(parts, total)
    return [total // parts + (1 if i < total % parts else 0) for i in range(parts)]


def ring_plan(costs, count, latency):
    ready = {(c, 0): 0.0 for c in range(len(costs))}
    free, plan, landed = 0.0, [], {}
    while ready:
        at_hand = [k for k in ready if ready[k] <= free]
        if not at_hand:
            free = min(ready.values())
            continue
        c, s = min(at_hand, key=lambda k: (k[0], -k[1]))
        begin = free
        del ready[(c, s)]
        free = free + costs[c]
        landed[(c, s)] = free + latency
        plan.append((begin, c, s))
        if s + 1 < count - 1:
            ready[(c, s + 1)] = free + latency
    for c in range(len(costs)):
        plan.append((landed[(c, count - 2)], c, count - 1))
    passed, free = {}, 0.0
    for when, c, s in sorted((landed[k], k[0], k[1] + 1) for k in landed):
        free = max(free, when) + costs[c]
        passed[(c, s)] = free + latency
    return sorted(plan), passed


def layer_body(dims, *refs):
    (n, copies, tp, rows, model, dc, rec, blocks, brows, width, ff, hid, col) = dims
    tokens, weights, (
        out_scale, down_scale, gate_scale, in_scale, recur_scale, inject_scale, swish_scale, up_scale,
        gain1, gain2, taps, decay_param, shift, out,
        Fg, Fi, Fr, Fj, Fo, Fs, Fu, Fd,
        Wp, Wb, Wo, Wf, Wd, X, H, N, UG, M, T, R1, R2, A, S, SV, SP, Z,
        z_send, z_recv, y_send, y_recv, own_sem, tok_sem,
        x_send, x_recv, r1_send, r1_recv, h_send, h_recv, r2_send, r2_recv, s_send, s_recv,
    ) = refs[0], refs[1:9], refs[9:]
    g, f, t = lax.axis_index("grp"), lax.axis_index("fs"), lax.axis_index("tp")
    krows = model // n

    barrier = pltpu.get_barrier_semaphore()
    for axis, count, here in (("fs", n, f), ("grp", copies, g), ("tp", tp, t)):
        for k in range(1, count):
            pl.semaphore_signal(
                barrier, inc=1, device_id={axis: lax.rem(here + k, count)}, device_id_type=MESH
            )

    def remote(src, dst, send, recv, axis, index):
        return pltpu.make_async_remote_copy(
            src_ref=src, dst_ref=dst, send_sem=send, recv_sem=recv,
            device_id={axis: index}, device_id_type=MESH,
        )

    staged = (Fi, Fr, Fj, Fg, Fo, Fs, Fu, Fd)
    loads = {}
    for k, (source, place) in sorted(enumerate(zip(weights, staged)), key=lambda e: (e[0] not in (1, 2), e[0])):
        loads[k] = pltpu.make_async_copy(source, place, own_sem.at[k])
        loads[k].start()
    tok = pltpu.make_async_copy(tokens, X.at[t], tok_sem.at[0])
    tok.start()

    def loaded(*which):
        for k in which:
            if k in loads:
                loads.pop(k).wait()

    def by_tiles(total, step, run):
        def tile(i, _):
            run(pl.multiple_of(i * step, step))
            return 0

        lax.fori_loop(0, total // step, tile, 0)

    chunks, tags = [], {}

    def by_rows(buf, first, wide, parts):
        per = krows // copies

        def view(owner, share):
            return buf.at[pl.ds(pl.multiple_of(owner * krows + share * per, per), per), pl.ds(first, wide)]

        def fill():
            loaded(*(k for k, _, _, _ in parts))

            def tile(at):
                here = pl.ds(pl.multiple_of(f * krows + at, TILE), TILE)
                for k, source, start, many in parts:
                    got = staged[k][pl.ds(at, TILE), source : source + many].astype(jnp.bfloat16)
                    buf[here, start : start + many] = got

            by_tiles(krows, TILE, tile)

        return view, fill, per * wide

    def by_columns(buf, k, scale, first, wide):
        deep, height = buf.shape[0], staged[k].shape[0]
        per = deep // copies

        def view(owner, share):
            return buf.at[
                pl.ds(pl.multiple_of(share * per, per), per),
                pl.ds(pl.multiple_of(owner * col + first, LANES), wide),
            ]

        def fill():
            loaded(k)
            lanes = pl.ds(pl.multiple_of(f * col + first, LANES), wide)

            def tile(at):
                got = staged[k][pl.ds(at, TILE), first : first + wide] * scale[:, first : first + wide]
                buf[pl.ds(at, TILE), lanes] = got.astype(jnp.bfloat16)

            by_tiles(height, TILE, tile)
            if deep > height:
                buf[height:deep, lanes] = jnp.zeros((deep - height, wide), jnp.bfloat16)

        return view, fill, per * wide

    def by_blocks():
        per = 2 * width // copies

        def view(owner, share):
            return Wb.at[
                :, pl.ds(pl.multiple_of(owner * brows, brows), brows),
                pl.ds(pl.multiple_of(share * per, per), per),
            ]

        def fill():
            loaded(1, 2)
            here = pl.ds(pl.multiple_of(f * brows, brows), brows)
            Wb[:, here, :width] = Fr[...].astype(jnp.bfloat16)
            Wb[:, here, width:] = Fj[...].astype(jnp.bfloat16)

        return view, fill, blocks * brows * per

    def by_pairs(first, pairs):
        parts = []
        for i in range(first, first + pairs):
            many = min(LANES, ff - i * LANES)
            parts.append((5, i * LANES, 2 * i * LANES, many))
            parts.append((6, i * LANES, (2 * i + 1) * LANES, many))
        return by_rows(Wf, first * 2 * LANES, pairs * 2 * LANES, parts)

    if hid > ff:
        own_rows = pl.ds(pl.multiple_of(f * krows, krows), krows)
        Wf[own_rows, 2 * (hid - LANES) : 2 * hid] = jnp.zeros((krows, 2 * LANES), jnp.bfloat16)

    def add(tag, chunk):
        tags[tag] = len(chunks)
        chunks.append(chunk)

    add("blk", by_blocks())
    add("in", by_rows(Wp, rec, rec, [(0, 0, rec, rec)]))
    add("gate", by_rows(Wp, 0, rec, [(3, 0, 0, rec)]))
    add("out", by_columns(Wo, 4, out_scale, 0, col))
    ff_groups, first = [], 0
    for pairs in shares(hid // LANES, 4):
        add(("ff", len(ff_groups)), by_pairs(first, pairs))
        ff_groups.append((first, pairs))
        first += pairs
    dn_groups, first = [], 0
    for lanes in shares(col // LANES, 3):
        add(("dn", len(dn_groups)), by_columns(Wd, 7, down_scale, first * LANES, lanes * LANES))
        dn_groups.append((first * LANES, lanes * LANES))
        first += lanes

    chunks[0][1]()
    pl.semaphore_wait(barrier, (n - 1) + (copies - 1) + (tp - 1))

    drains = []

    def send(copy, when=None):
        if when is None:
            copy.start()
        else:
            @pl.when(when)
            def _():
                copy.start()

        drains.append((copy, when))

    def z_copy(c, owner, side):
        view = chunks[c][0](owner, g)
        return remote(
            view, view, z_send.at[side, c, owner], z_recv.at[c, owner], "fs",
            jnp.clip(f - 1 if side else f + 1, 0, n - 1),
        )

    def y_copy(c, owner, other, share):
        view = chunks[c][0](owner, share)
        return remote(
            view, view, y_send.at[c, owner, other - 1], y_recv.at[c, owner, other - 1],
            "grp", lax.rem(g + other, copies),
        )

    def line_step(c, s):
        if s == 0 and c:
            chunks[c][1]()
        for side in range(2):
            owner = jnp.clip(f + s if side else f - s, 0, n - 1)
            here = f + s < n if side else f >= s
            onward = f > 0 if side else f < n - 1
            if s:
                @pl.when(here)
                def _():
                    z_copy(c, owner, side).wait_recv()
                    for other in range(1, copies):
                        y_copy(c, owner, other, g).start()

                for other in range(1, copies):
                    drains.append((y_copy(c, owner, other, g), here))
            send(z_copy(c, owner, side), jnp.logical_and(here, onward))

    def settled(c, owner):
        for other in range(1, copies):
            y_copy(c, owner, other, lax.rem(g - other + copies, copies)).wait_recv()

    def gathered(c):
        for k in range(1, n):
            settled(c, lax.rem(f + k, n))

    def nearest(m):
        near = jnp.minimum(f, n - 1 - f)
        two = (m + 1) // 2
        paired = f - two if m % 2 else f + two
        single = jnp.where(f < n - 1 - f, f + (m - near), f - (m - near))
        return jnp.where(m <= 2 * near, paired, single)

    def spread(source, buf, sends, recvs):
        for k in range(1, tp):
            send(remote(source, buf.at[t], sends.at[k - 1], recvs.at[k - 1], "tp", lax.rem(t + k, tp)))

    def spread_land(buf, sends, recvs):
        for k in range(1, tp):
            place = buf.at[lax.rem(t - k + tp, tp)]
            remote(place, place, sends.at[k - 1], recvs.at[k - 1], "tp", lax.rem(t + k, tp)).wait_recv()

    spread(tokens, X, x_send, x_recv)

    def send_scales():
        def placed(scale, wide):
            many = scale.shape[1]
            Z[:, :wide] = jnp.zeros((8, wide), jnp.float32)
            Z[:, :many] = jnp.broadcast_to(scale, (8, many))
            return pltpu.roll(Z[:, :wide], f * many, 1)[0:1]

        S[f, :, 0:rec] = placed(gate_scale[...], rec)
        S[f, :, rec : 2 * rec] = placed(in_scale[...], rec)
        for base, scale in ((2 * rec, recur_scale), (3 * rec, inject_scale)):
            for block in range(blocks):
                at = base + block * width
                S[f, :, at : at + width] = placed(scale[block : block + 1, :], width)
        for half, scale in enumerate((swish_scale, up_scale)):
            whole = placed(scale[...], hid)
            for i in range(hid // LANES):
                at = 4 * rec + (2 * i + half) * LANES
                S[f, :, at : at + LANES] = whole[:, i * LANES : (i + 1) * LANES]
        for k in range(1, n):
            send(remote(S.at[f], S.at[f], s_send.at[k - 1], s_recv.at[k - 1], "fs", lax.rem(f + k, n)))
        lost = -decay_param[...]
        u = jnp.exp(-jnp.abs(lost))
        z = u / (2.0 + u)
        square, tail = z * z, 0.0
        for odd in range(17, 0, -2):
            tail = tail * square + 1.0 / odd
        SP[...] = jnp.maximum(lost, 0.0) + 2.0 * z * tail

    def norm(buf, gain):
        def tile(i, _):
            here = pl.ds(pl.multiple_of(i * SEQ_LEN, SEQ_LEN), SEQ_LEN)
            parts = [buf[p, here, :].astype(jnp.float32) for p in range(tp)]
            total = sum(jnp.sum(v * v, axis=-1, keepdims=True) for v in parts)
            factor = lax.rsqrt(total / model + eps)
            for p in range(tp):
                lanes = slice(p * dc, (p + 1) * dc)
                N[here, lanes] = (parts[p] * factor * gain[:, lanes]).astype(jnp.bfloat16)
            return 0

        lax.fori_loop(0, rows // SEQ_LEN, tile, 0)

    def first_norm():
        tok.wait()
        spread_land(X, x_send, x_recv)
        norm(X, gain1)

    def project(tag, first):
        def run():
            gathered(tags[tag])

            def tile(i, _):
                lanes = pl.ds(pl.multiple_of(first + i * 256, LANES), 256)
                summed = jnp.dot(N[...], Wp[:, lanes], preferred_element_type=jnp.float32)
                UG[:, lanes] = (summed * SV[:, lanes]).astype(jnp.bfloat16)
                return 0

            lax.fori_loop(0, rec // 256, tile, 0)

        return run

    def scale_sum():
        for k in range(1, n):
            place = S.at[lax.rem(f - k + n, n)]
            remote(place, place, s_send.at[k - 1], s_recv.at[k - 1], "fs", lax.rem(f + k, n)).wait_recv()
        total = S[0]
        for o in range(1, n):
            total = total + S[o]
        SV[...] = total

    def recurrence():
        gathered(tags["blk"])
        position = lax.broadcasted_iota(jnp.int32, (SEQ_LEN, width), 0)
        square = (SEQ_LEN, SEQ_LEN)
        diagonal = lax.broadcasted_iota(jnp.int32, square, 0) == lax.broadcasted_iota(jnp.int32, square, 1)

        def sequence(i, _):
            here = pl.ds(pl.multiple_of(i * SEQ_LEN, SEQ_LEN), SEQ_LEN)
            along = jnp.broadcast_to(shift[pl.ds(i, 1), :], (SEQ_LEN, SEQ_LEN))
            moved_by = jnp.sum(jnp.where(diagonal, along, 0.0), axis=1, keepdims=True)
            for block in range(blocks):
                lanes = slice(block * width, (block + 1) * width)
                at = lambda base: slice(base + block * width, base + (block + 1) * width)
                branch = UG[here, at(rec)].astype(jnp.float32)
                summed = branch * taps[0:1, lanes]
                for offset in range(1, TAPS):
                    moved = jnp.where(position >= offset, pltpu.roll(branch, offset, 0), 0.0)
                    summed = summed + moved * taps[offset : offset + 1, lanes]
                conv = summed.astype(jnp.bfloat16)
                sums = jnp.dot(conv, Wb[block], preferred_element_type=jnp.float32)
                recur = jax.nn.sigmoid(sums[:, :width] * SV[:, at(2 * rec)])
                inject = jax.nn.sigmoid(sums[:, width:] * SV[:, at(3 * rec)])
                log_keep = -8.0 * recur * SP[:, lanes] + moved_by
                twice = 2.0 * log_keep
                near = -twice * (
                    1.0
                    + twice * (0.5 + twice * (1.0 / 6 + twice * (1.0 / 24 + twice * (1.0 / 120))))
                )
                lost = jnp.where(twice > -0.125, near, 1.0 - jnp.exp(twice))
                factor = jnp.where(position == 0, 1.0, jnp.sqrt(lost))
                state = conv.astype(jnp.float32) * inject * factor
                keep = jnp.exp(log_keep)
                reach = 1
                while reach < SEQ_LEN:
                    inside = position >= reach
                    state = state + keep * jnp.where(inside, pltpu.roll(state, reach, 0), 0.0)
                    keep = keep * jnp.where(inside, pltpu.roll(keep, reach, 0), 1.0)
                    reach *= 2
                gate = UG[here, lanes].astype(jnp.float32)
                M[here, lanes] = (jax.nn.gelu(gate) * state).astype(jnp.bfloat16)
            return 0

        lax.fori_loop(0, rows // SEQ_LEN, sequence, 0)

    mixed = []

    def mix_out():
        gathered(tags["out"])
        for k in list(range(1, tp)) + [0]:
            peer = lax.rem(t + k, tp)
            lanes = pl.ds(pl.multiple_of(peer * dc, dc), dc)
            T[:, lanes] = jnp.dot(M[...], Wo[:, lanes], preferred_element_type=jnp.float32).astype(jnp.bfloat16)
            if k:
                mixed.append(
                    remote(T.at[:, lanes], R1.at[k - 1], r1_send.at[k - 1], r1_recv.at[k - 1], "tp", peer)
                )
                mixed[-1].start()

    def hidden():
        for k in range(1, tp):
            place = R1.at[k - 1]
            remote(place, place, r1_send.at[k - 1], r1_recv.at[k - 1], "tp", lax.rem(t + k, tp)).wait_recv()

        def tile(i, _):
            here = pl.ds(pl.multiple_of(i * SEQ_LEN, SEQ_LEN), SEQ_LEN)
            total = T[here, pl.ds(pl.multiple_of(t * dc, dc), dc)].astype(jnp.float32)
            for k in range(1, tp):
                total = total + R1[k - 1, here, :].astype(jnp.float32)
            H[t, here, :] = (X[t, here, :].astype(jnp.float32) + total).astype(jnp.bfloat16)
            return 0

        lax.fori_loop(0, rows // SEQ_LEN, tile, 0)
        spread(H.at[t], H, h_send, h_recv)

    def second_norm():
        spread_land(H, h_send, h_recv)
        norm(H, gain2)

    def activate(index, first, pairs, opens):
        def run():
            if opens:
                gathered(tags[("ff", index)])

            def tile(i, _):
                both = pl.ds(pl.multiple_of((first + i) * 2 * LANES, 2 * LANES), 2 * LANES)
                cols = pl.ds(pl.multiple_of(4 * rec + (first + i) * 2 * LANES, LANES), 2 * LANES)
                summed = jnp.dot(N[...], Wf[:, both], preferred_element_type=jnp.float32)
                summed = summed * SV[:, cols]
                one = pl.ds(pl.multiple_of((first + i) * LANES, LANES), LANES)
                A[:, one] = (jax.nn.silu(summed[:, :LANES]) * summed[:, LANES:]).astype(jnp.bfloat16)
                return 0

            lax.fori_loop(0, pairs, tile, 0)

        return run

    pieces = []

    def down(index, s):
        first, wide = dn_groups[index]

        def run():
            while mixed:
                mixed.pop().wait_send()
            owner = nearest(s)
            if s:
                settled(tags[("dn", index)], owner)
            start = owner * col + first
            lanes = pl.ds(pl.multiple_of(start, LANES), wide)
            peer = start // dc
            inner = start - peer * dc
            T[:, lanes] = jnp.dot(A[...], Wd[:, lanes], preferred_element_type=jnp.float32).astype(jnp.bfloat16)

            def piece():
                return remote(
                    T.at[:, lanes], R2.at[t, :, pl.ds(pl.multiple_of(inner, LANES), wide)],
                    r2_send.at[index, s], r2_recv.at[t, inner // LANES], "tp", peer,
                )

            @pl.when(peer != t)
            def _():
                piece().start()

            pieces.append((peer, piece))

        return run

    def finish():
        for k in range(1, tp):
            peer = lax.rem(t + k, tp)
            for part in range(dc // col):
                for first, wide in dn_groups:
                    inner = part * col + first
                    place = R2.at[peer, :, pl.ds(inner, wide)]
                    remote(place, place, r2_send.at[0, 0], r2_recv.at[peer, inner // LANES], "tp", peer).wait_recv()

        def tile(i, _):
            here = pl.ds(pl.multiple_of(i * SEQ_LEN, SEQ_LEN), SEQ_LEN)
            total = T[here, pl.ds(pl.multiple_of(t * dc, dc), dc)].astype(jnp.float32)
            for k in range(1, tp):
                total = total + R2[lax.rem(t + k, tp), here, :].astype(jnp.float32)
            out[here, :] = (H[t, here, :].astype(jnp.float32) + total).astype(jnp.bfloat16)
            return 0

        lax.fori_loop(0, rows // SEQ_LEN, tile, 0)

    link = 2 * 2 / 91e3
    costs = [chunk[2] * link for chunk in chunks]
    ring, passed = ring_plan(costs, n, 5.0)
    events = [(when, 0, c, s, None) for when, c, s in ring]

    def ready(tag, s=None):
        return passed[(tags[tag], n - 1 if s is None else s)]

    clock = [0.0]

    def task(when, takes, run):
        clock[0] = max(clock[0], when)
        events.append((clock[0], 1, len(events), 0, run))
        clock[0] += takes

    across = tp * rows * dc * link / 2
    task(3.0, 1.0, send_scales)
    task(20.0, 0.5, scale_sum)
    task(across, 3.0, first_norm)
    task(ready("in"), 2.0, project("in", rec))
    task(ready("gate"), 2.0, project("gate", 0))
    task(ready("blk"), 6.0, recurrence)
    task(ready("out"), 4.0, mix_out)
    task(clock[0] + across, 2.0, hidden)
    task(clock[0] + across, 3.0, second_norm)
    for index, (first, pairs) in enumerate(ff_groups):
        for start in range(0, pairs, 2):
            many = min(2, pairs - start)
            task(ready(("ff", index)), 1.0 * many, activate(index, first + start, many, start == 0))
    last = [(ready(("dn", index), s) if s else 0.0, index, s) for index in range(len(dn_groups)) for s in range(n)]
    for when, index, s in sorted(last):
        task(when, 1.3, down(index, s))
    for _, kind, c, s, run in sorted(events, key=lambda e: e[:4]):
        if kind == 0:
            line_step(c, s)
        else:
            run()
    finish()
    for copy, when in drains:
        if when is None:
            copy.wait_send()
        else:
            @pl.when(when)
            def _(copy=copy):
                copy.wait_send()

    for peer, piece in pieces:
        @pl.when(peer != t)
        def _(piece=piece):
            piece().wait_send()


def on_device(
    tokens,
    recurrent_norm_gain,
    channel_norm_gain,
    gate_projection_weight,
    gate_column_scale,
    input_projection_weight,
    input_column_scale,
    convolution_kernel,
    recurrence_gate_weight,
    recurrence_column_scale,
    input_gate_weight,
    input_gate_column_scale,
    channel_decay_param,
    position_decay_shift,
    output_projection_weight,
    output_column_scale,
    mixer_gate_weight,
    mixer_gate_column_scale,
    up_projection_weight,
    up_column_scale,
    down_projection_weight,
    down_column_scale,
):
    n, copies, tp = (lax.axis_size(axis) for axis in ("fs", "grp", "tp"))
    rows, dc = tokens.shape
    model = dc * tp
    krows, rec = gate_projection_weight.shape
    blocks, brows, width = recurrence_gate_weight.shape
    ff = mixer_gate_weight.shape[1]
    hid = -(-ff // LANES) * LANES
    col = output_projection_weight.shape[1]

    weights = (
        input_projection_weight,
        recurrence_gate_weight,
        input_gate_weight,
        gate_projection_weight,
        output_projection_weight,
        mixer_gate_weight,
        up_projection_weight,
        down_projection_weight,
    )

    dims = (n, copies, tp, rows, model, dc, rec, blocks, brows, width, ff, hid, col)
    chunk_count = 4 + len(shares(hid // LANES, 4)) + len(shares(col // LANES, 3))
    here = pl.BlockSpec(memory_space=pltpu.VMEM)
    away = pl.BlockSpec(memory_space=pl.ANY)
    bf = lambda *shape: pltpu.VMEM(shape, jnp.bfloat16)
    dma = lambda *shape: pltpu.SemaphoreType.DMA(shape)
    flops = 2 * rows * (model * (2 * rec + 2 * hid) + rec * 2 * width + rec * model + hid * model)
    return pl.pallas_call(
        lambda *refs: layer_body(dims, *refs),
        out_shape=jax.ShapeDtypeStruct((rows, dc), jnp.bfloat16),
        in_specs=[away] * 9 + [here] * 13,
        out_specs=here,
        scratch_shapes=[
            pltpu.VMEM(gate_projection_weight.shape, jnp.float32),
            pltpu.VMEM(input_projection_weight.shape, jnp.float32),
            pltpu.VMEM(recurrence_gate_weight.shape, jnp.float32),
            pltpu.VMEM(input_gate_weight.shape, jnp.float32),
            pltpu.VMEM(output_projection_weight.shape, jnp.float32),
            pltpu.VMEM(mixer_gate_weight.shape, jnp.float32),
            pltpu.VMEM(up_projection_weight.shape, jnp.float32),
            pltpu.VMEM(down_projection_weight.shape, jnp.float32),
            bf(model, 2 * rec),
            bf(blocks, n * brows, 2 * width),
            bf(rec, model),
            bf(model, 2 * hid),
            bf(hid, model),
            bf(tp, rows, dc),
            bf(tp, rows, dc),
            bf(rows, model),
            bf(rows, 2 * rec),
            bf(rows, rec),
            bf(rows, model),
            bf(tp - 1, rows, dc),
            bf(tp, rows, dc),
            bf(rows, hid),
            pltpu.VMEM((n, 1, 4 * rec + 2 * hid), jnp.float32),
            pltpu.VMEM((1, 4 * rec + 2 * hid), jnp.float32),
            pltpu.VMEM((1, rec), jnp.float32),
            pltpu.VMEM((8, max(rec, hid)), jnp.float32),
            dma(2, chunk_count, n),
            dma(chunk_count, n),
            dma(chunk_count, n, copies - 1),
            dma(chunk_count, n, copies - 1),
            dma(len(weights)),
            dma(1),
            dma(tp - 1),
            dma(tp - 1),
            dma(tp - 1),
            dma(tp - 1),
            dma(tp - 1),
            dma(tp - 1),
            dma(len(shares(col // LANES, 3)), n),
            dma(tp, dc // LANES),
            dma(n - 1),
            dma(n - 1),
        ],
        compiler_params=pltpu.CompilerParams(
            collective_id=0, has_side_effects=True, vmem_limit_bytes=67_043_328
        ),
        cost_estimate=pl.CostEstimate(flops=flops, bytes_accessed=8 * rows * model, transcendentals=0),
    )(
        tokens,
        *weights,
        output_column_scale[None, :],
        down_column_scale[None, :],
        gate_column_scale[None, :],
        input_column_scale[None, :],
        recurrence_column_scale,
        input_gate_column_scale,
        mixer_gate_column_scale[None, :],
        up_column_scale[None, :],
        recurrent_norm_gain[None, :],
        channel_norm_gain[None, :],
        convolution_kernel,
        channel_decay_param[None, :],
        position_decay_shift.reshape(-1, SEQ_LEN),
    )


def solution(mesh):
    placed = (
        P(("grp", "fs"), "tp"),
        P(),
        P(),
        P("fs", "tp"),
        P(("tp", "fs")),
        P("fs", "tp"),
        P(("tp", "fs")),
        P(None, "tp"),
        P("tp", "fs", None),
        P("tp", "fs"),
        P("tp", "fs", None),
        P("tp", "fs"),
        P("tp"),
        P(("grp", "fs")),
        P("tp", "fs"),
        P("fs"),
        P("fs", "tp"),
        P(("tp", "fs")),
        P("fs", "tp"),
        P(("tp", "fs")),
        P("tp", "fs"),
        P("fs"),
    )
    return jax.shard_map(
        on_device, mesh=mesh, in_specs=placed, out_specs=P(("grp", "fs"), "tp"), check_vma=False
    )
```

```python
import jax
import jax.numpy as jnp
from jax import lax
from jax.experimental import pallas as pl
from jax.experimental.pallas import tpu as pltpu
from jax.sharding import PartitionSpec as P

TAPS = 4
SEQ_LEN = 128
LANES = 128
TILE = 64
MESH = pl.DeviceIdType.MESH

eps = 1e-06


def shares(total, parts):
    parts = min(parts, total)
    return [total // parts + (1 if i < total % parts else 0) for i in range(parts)]


def parted(total, parts):
    spans, first = [], 0
    for many in shares(total, parts):
        spans.append((first, many))
        first += many
    return spans


def solo_rows(deep):
    return deep * 3 // 8 // LANES * LANES


def first_cuts(width):
    cuts = []
    for k in (1, 1, 2):
        if sum(cuts) + k * LANES < width:
            cuts.append(k * LANES)
    return cuts + [width - sum(cuts)]


def ring_plan(costs, solo, count, latency):
    ready = {(c, 0): 0.0 for c in range(len(costs))}
    free, plan, landed = 0.0, [], {}
    while ready:
        at_hand = [k for k in ready if ready[k] <= free]
        if not at_hand:
            free = min(ready.values())
            continue
        c, s = min(at_hand, key=lambda k: (k[0], -k[1]))
        begin = free
        del ready[(c, s)]
        free = free + costs[c]
        landed[(c, s)] = free + (2.5 if free < 10.0 else latency)
        plan.append((begin, c, s))
        if s + 1 < count - 1:
            ready[(c, s + 1)] = landed[(c, s)]
    for c in range(len(costs)):
        plan.append((landed[(c, count - 2)], c, count - 1))
    passed, free = {}, 0.0
    for when, c, s in sorted((landed[k], k[0], k[1] + 1) for k in landed):
        if solo[c]:
            passed[(c, s)] = when
        else:
            free = max(free, when) + costs[c]
            passed[(c, s)] = free + latency
    return sorted(plan), passed


def layer_body(dims, *refs):
    (n, copies, tp, rows, model, dc, rec, blocks, brows, width, ff, hid, col) = dims
    tokens, weights, (
        out_scale, down_scale, gate_scale, in_scale, recur_scale, inject_scale, swish_scale, up_scale,
        gain1, gain2, taps, decay_param, shift, out,
        Fg, Fi, Fr, Fj, Fo, Fs, Fu, Fd,
        Wp, Wb, Wo, Wf, Wd, X, H, N, UG, M, T, R1, R2, A, S, SV, SP, Z, B, V, E,
        z_send, z_recv, y_send, y_recv, own_sem, tok_sem,
        x_send, x_recv, r1_send, r1_recv, h_send, h_recv, r2_send, r2_recv, s_send, s_recv,
        b_send, b_recv, out_sem,
    ) = refs[0], refs[1:9], refs[9:]
    g, f, t = lax.axis_index("grp"), lax.axis_index("fs"), lax.axis_index("tp")
    krows = model // n

    barrier = pltpu.get_barrier_semaphore()
    for axis, count, here in (("fs", n, f), ("grp", copies, g), ("tp", tp, t)):
        for k in range(1, count):
            pl.semaphore_signal(
                barrier, inc=1, device_id={axis: lax.rem(here + k, count)}, device_id_type=MESH
            )

    def remote(src, dst, send, recv, axis, index):
        return pltpu.make_async_remote_copy(
            src_ref=src, dst_ref=dst, send_sem=send, recv_sem=recv,
            device_id={axis: index}, device_id_type=MESH,
        )

    staged = (Fi, Fr, Fj, Fg, Fo, Fs, Fu, Fd)
    loads = {}
    for k, (source, place) in sorted(enumerate(zip(weights, staged)), key=lambda e: (e[0] not in (1, 2), e[0])):
        loads[k] = pltpu.make_async_copy(source, place, own_sem.at[k])
        loads[k].start()
    tok = pltpu.make_async_copy(tokens, X.at[t], tok_sem.at[0])
    tok.start()

    def loaded(*which):
        for k in which:
            if k in loads:
                loads.pop(k).wait()

    def by_tiles(total, step, run):
        def tile(i, _):
            run(pl.multiple_of(i * step, step))
            return 0

        lax.fori_loop(0, total // step, tile, 0)

    chunks, tags = [], {}

    def by_rows(buf, first, wide, parts):
        per = krows // copies

        def view(owner, share):
            return buf.at[pl.ds(pl.multiple_of(owner * krows + share * per, per), per), pl.ds(first, wide)]

        def fill():
            loaded(*(k for k, _, _, _ in parts))

            def tile(at):
                here = pl.ds(pl.multiple_of(f * krows + at, TILE), TILE)
                for k, source, start, many in parts:
                    got = staged[k][pl.ds(at, TILE), source : source + many].astype(jnp.bfloat16)
                    buf[here, start : start + many] = got

            by_tiles(krows, TILE, tile)

        return view, fill, per * wide, False

    def by_columns(buf, k, scale, first, wide, top=0, bottom=None, solo=False):
        deep = (buf.shape[0] if bottom is None else bottom) - top
        height = min(deep, staged[k].shape[0] - top)
        per = deep if solo else deep // copies

        def view(owner, share):
            start = top if solo else pl.multiple_of(top + share * per, 16)
            return buf.at[pl.ds(start, per), pl.ds(pl.multiple_of(owner * col + first, LANES), wide)]

        def fill():
            loaded(k)
            lanes = pl.ds(pl.multiple_of(f * col + first, LANES), wide)

            def tile(at):
                here = pl.ds(pl.multiple_of(top + at, TILE), TILE)
                got = staged[k][here, first : first + wide] * scale[:, first : first + wide]
                buf[here, lanes] = got.astype(jnp.bfloat16)

            by_tiles(height, TILE, tile)
            if deep > height:
                buf[top + height : top + deep, lanes] = jnp.zeros((deep - height, wide), jnp.bfloat16)

        return view, fill, per * wide, solo

    def by_blocks():
        per = 2 * width // copies

        def view(owner, share):
            return Wb.at[
                :, pl.ds(pl.multiple_of(owner * brows, brows), brows),
                pl.ds(pl.multiple_of(share * per, per), per),
            ]

        def fill():
            loaded(1, 2)
            here = pl.ds(pl.multiple_of(f * brows, brows), brows)
            Wb[:, here, :width] = Fr[...].astype(jnp.bfloat16)
            Wb[:, here, width:] = Fj[...].astype(jnp.bfloat16)

        return view, fill, blocks * brows * per, False

    def by_pairs(first, pairs):
        parts = []
        for i in range(first, first + pairs):
            many = min(LANES, ff - i * LANES)
            parts.append((5, i * LANES, 2 * i * LANES, many))
            parts.append((6, i * LANES, (2 * i + 1) * LANES, many))
        return by_rows(Wf, first * 2 * LANES, pairs * 2 * LANES, parts)

    if hid > ff:
        own_rows = pl.ds(pl.multiple_of(f * krows, krows), krows)
        Wf[own_rows, 2 * (hid - LANES) : 2 * hid] = jnp.zeros((krows, 2 * LANES), jnp.bfloat16)

    def add(tag, chunk):
        tags[tag] = len(chunks)
        chunks.append(chunk)

    add("blk", by_blocks())
    def add_projection(tag, k, base, cuts):
        start = 0
        for i, wide in enumerate(cuts):
            add((tag, i), by_rows(Wp, base + start, wide, [(k, start, base + start, wide)]))
            start += wide

    in_cuts, gate_cuts = first_cuts(rec), [LANES * k for k in shares(rec // LANES, 2)]
    add_projection("in", 0, rec, in_cuts)
    add_projection("gate", 3, 0, gate_cuts)
    add("out", by_columns(Wo, 4, out_scale, 0, col))
    ff_groups, first = [], 0
    for pairs in shares(hid // LANES, 4):
        add(("ff", len(ff_groups)), by_pairs(first, pairs))
        ff_groups.append((first, pairs))
        first += pairs
    dn_groups, first = [], 0
    for lanes in shares(col // LANES, 3):
        index, at, wide = len(dn_groups), first * LANES, lanes * LANES
        cut = solo_rows(hid) if index == len(shares(col // LANES, 3)) - 1 else 0
        add(("dn", index), by_columns(Wd, 7, down_scale, at, wide, cut, hid))
        if cut:
            add("solo", by_columns(Wd, 7, down_scale, at, wide, 0, cut, True))
        dn_groups.append((first * LANES, lanes * LANES))
        first += lanes

    chunks[0][1]()
    pl.semaphore_wait(barrier, (n - 1) + (copies - 1) + (tp - 1))

    drains = []

    def send(copy, when=None):
        if when is None:
            copy.start()
        else:
            @pl.when(when)
            def _():
                copy.start()

        drains.append((copy, when))

    def z_copy(c, owner, side):
        view = chunks[c][0](owner, g)
        return remote(
            view, view, z_send.at[side, c, owner], z_recv.at[c, owner], "fs",
            jnp.clip(f - 1 if side else f + 1, 0, n - 1),
        )

    def y_copy(c, owner, other, share):
        view = chunks[c][0](owner, share)
        return remote(
            view, view, y_send.at[c, owner, other - 1], y_recv.at[c, owner, other - 1],
            "grp", lax.rem(g + other, copies),
        )

    def passing(c):
        return range(1, 1 if chunks[c][3] else copies)

    def line_step(c, s):
        if s == 0 and c:
            chunks[c][1]()
        for side in range(2):
            owner = jnp.clip(f + s if side else f - s, 0, n - 1)
            here = f + s < n if side else f >= s
            onward = f > 0 if side else f < n - 1
            if s:
                @pl.when(here)
                def _():
                    z_copy(c, owner, side).wait_recv()
                    for other in passing(c):
                        y_copy(c, owner, other, g).start()

                for other in passing(c):
                    drains.append((y_copy(c, owner, other, g), here))
            send(z_copy(c, owner, side), jnp.logical_and(here, onward))

    def settled(c, owner):
        for other in passing(c):
            y_copy(c, owner, other, lax.rem(g - other + copies, copies)).wait_recv()

    def gathered(c):
        for k in range(1, n):
            settled(c, lax.rem(f + k, n))

    def nearest(m):
        near = jnp.minimum(f, n - 1 - f)
        two = (m + 1) // 2
        paired = f - two if m % 2 else f + two
        single = jnp.where(f < n - 1 - f, f + (m - near), f - (m - near))
        return jnp.where(m <= 2 * near, paired, single)

    def spread(source, buf, sends, recvs):
        for k in range(1, tp):
            send(remote(source, buf.at[t], sends.at[k - 1], recvs.at[k - 1], "tp", lax.rem(t + k, tp)))

    def spread_land(buf, sends, recvs):
        for k in range(1, tp):
            place = buf.at[lax.rem(t - k + tp, tp)]
            remote(place, place, sends.at[k - 1], recvs.at[k - 1], "tp", lax.rem(t + k, tp)).wait_recv()

    spread(tokens, X, x_send, x_recv)

    def send_scales():
        def placed(scale, wide):
            many = scale.shape[-1]
            scale = scale.reshape(1, many)
            Z[:, :wide] = jnp.zeros((8, wide), jnp.float32)
            Z[:, :many] = jnp.broadcast_to(scale, (8, many))
            return pltpu.roll(Z[:, :wide], f * many, 1)[0:1]

        S[f, :, 0:rec] = placed(gate_scale[...], rec)
        S[f, :, rec : 2 * rec] = placed(in_scale[...], rec)
        for base, scale in ((2 * rec, recur_scale), (3 * rec, inject_scale)):
            for block in range(blocks):
                at = base + block * width
                S[f, :, at : at + width] = placed(scale[block : block + 1, :], width)
        for half, scale in enumerate((swish_scale, up_scale)):
            whole = placed(scale[...], hid)
            for i in range(hid // LANES):
                at = 4 * rec + (2 * i + half) * LANES
                S[f, :, at : at + LANES] = whole[:, i * LANES : (i + 1) * LANES]
        for k in range(1, n):
            send(remote(S.at[f], S.at[f], s_send.at[k - 1], s_recv.at[k - 1], "fs", lax.rem(f + k, n)))
        lost = -decay_param[...]
        u = jnp.exp(-jnp.abs(lost))
        z = u / (2.0 + u)
        square, tail = z * z, 0.0
        for odd in range(17, 0, -2):
            tail = tail * square + 1.0 / odd
        SP[...] = jnp.maximum(lost, 0.0) + 2.0 * z * tail

    def norm(buf, gain):
        def tile(i, _):
            here = pl.ds(pl.multiple_of(i * SEQ_LEN, SEQ_LEN), SEQ_LEN)
            parts = [buf[p, here, :].astype(jnp.float32) for p in range(tp)]
            total = sum(jnp.sum(v * v, axis=-1, keepdims=True) for v in parts)
            factor = lax.rsqrt(total / model + eps)
            for p in range(tp):
                lanes = slice(p * dc, (p + 1) * dc)
                N[here, lanes] = (parts[p] * factor * gain[:, lanes]).astype(jnp.bfloat16)
            return 0

        lax.fori_loop(0, rows // SEQ_LEN, tile, 0)

    def first_norm():
        tok.wait()
        spread_land(X, x_send, x_recv)
        norm(X, gain1)

    def project(tag, cuts, first):
        def run():
            for i in range(len(cuts)):
                gathered(tags[(tag, i)])

            def tile(i, _):
                lanes = pl.ds(pl.multiple_of(first + i * 256, LANES), 256)
                summed = jnp.dot(N[...], Wp[:, lanes], preferred_element_type=jnp.float32)
                UG[:, lanes] = (summed * SV[:, lanes]).astype(jnp.bfloat16)
                return 0

            lax.fori_loop(0, rec // 256, tile, 0)

        return run

    def scale_sum():
        for k in range(1, n):
            place = S.at[lax.rem(f - k + n, n)]
            remote(place, place, s_send.at[k - 1], s_recv.at[k - 1], "fs", lax.rem(f + k, n)).wait_recv()
        total = S[0]
        for o in range(1, n):
            total = total + S[o]
        SV[...] = total

    def recurrence(first, many):
        return lambda: sequences_of(first, many)

    def sequences_of(first, many):
        if first == 0:
            gathered(tags["blk"])
        position = lax.broadcasted_iota(jnp.int32, (SEQ_LEN, width), 0)
        square = (SEQ_LEN, SEQ_LEN)
        diagonal = lax.broadcasted_iota(jnp.int32, square, 0) == lax.broadcasted_iota(jnp.int32, square, 1)

        def sequence(i, _):
            here = pl.ds(pl.multiple_of(i * SEQ_LEN, SEQ_LEN), SEQ_LEN)
            along = jnp.broadcast_to(shift[pl.ds(i, 1), :], (SEQ_LEN, SEQ_LEN))
            moved_by = jnp.sum(jnp.where(diagonal, along, 0.0), axis=1, keepdims=True)
            for block in range(blocks):
                lanes = slice(block * width, (block + 1) * width)
                at = lambda base: slice(base + block * width, base + (block + 1) * width)
                branch = UG[here, at(rec)].astype(jnp.float32)
                summed = branch * taps[0:1, lanes]
                for offset in range(1, TAPS):
                    moved = jnp.where(position >= offset, pltpu.roll(branch, offset, 0), 0.0)
                    summed = summed + moved * taps[offset : offset + 1, lanes]
                conv = summed.astype(jnp.bfloat16)
                sums = jnp.dot(conv, Wb[block], preferred_element_type=jnp.float32)
                recur = jax.nn.sigmoid(sums[:, :width] * SV[:, at(2 * rec)])
                inject = jax.nn.sigmoid(sums[:, width:] * SV[:, at(3 * rec)])
                log_keep = -8.0 * recur * SP[:, lanes] + moved_by
                twice = 2.0 * log_keep
                near = -twice * (
                    1.0
                    + twice * (0.5 + twice * (1.0 / 6 + twice * (1.0 / 24 + twice * (1.0 / 120))))
                )
                lost = jnp.where(twice > -0.125, near, 1.0 - jnp.exp(twice))
                factor = jnp.where(position == 0, 1.0, jnp.sqrt(lost))
                state = conv.astype(jnp.float32) * inject * factor
                keep = jnp.exp(log_keep)
                reach = 1
                while reach < SEQ_LEN:
                    inside = position >= reach
                    state = state + keep * jnp.where(inside, pltpu.roll(state, reach, 0), 0.0)
                    keep = keep * jnp.where(inside, pltpu.roll(keep, reach, 0), 1.0)
                    reach *= 2
                gate = UG[here, lanes].astype(jnp.float32)
                M[here, lanes] = (jax.nn.gelu(gate) * state).astype(jnp.bfloat16)
            return 0

        lax.fori_loop(first, first + many, sequence, 0)

    mixed = []

    def mix_out():
        gathered(tags["out"])
        for k in list(range(1, tp)) + [0]:
            peer = lax.rem(t + k, tp)
            lanes = pl.ds(pl.multiple_of(peer * dc, dc), dc)
            T[:, lanes] = jnp.dot(M[...], Wo[:, lanes], preferred_element_type=jnp.float32).astype(jnp.bfloat16)
            if k:
                mixed.append(
                    remote(T.at[:, lanes], R1.at[k - 1], r1_send.at[k - 1], r1_recv.at[k - 1], "tp", peer)
                )
                mixed[-1].start()

    def hidden():
        for k in range(1, tp):
            place = R1.at[k - 1]
            remote(place, place, r1_send.at[k - 1], r1_recv.at[k - 1], "tp", lax.rem(t + k, tp)).wait_recv()

        def tile(i, _):
            here = pl.ds(pl.multiple_of(i * SEQ_LEN, SEQ_LEN), SEQ_LEN)
            total = T[here, pl.ds(pl.multiple_of(t * dc, dc), dc)].astype(jnp.float32)
            for k in range(1, tp):
                total = total + R1[k - 1, here, :].astype(jnp.float32)
            H[t, here, :] = (X[t, here, :].astype(jnp.float32) + total).astype(jnp.bfloat16)
            return 0

        lax.fori_loop(0, rows // SEQ_LEN, tile, 0)
        spread(H.at[t], H, h_send, h_recv)

    def second_norm():
        spread_land(H, h_send, h_recv)
        norm(H, gain2)

    def activate(index, first, pairs, opens):
        def run():
            if opens:
                gathered(tags[("ff", index)])

            def tile(i, _):
                both = pl.ds(pl.multiple_of((first + i) * 2 * LANES, 2 * LANES), 2 * LANES)
                cols = pl.ds(pl.multiple_of(4 * rec + (first + i) * 2 * LANES, LANES), 2 * LANES)
                summed = jnp.dot(N[...], Wf[:, both], preferred_element_type=jnp.float32)
                summed = summed * SV[:, cols]
                one = pl.ds(pl.multiple_of((first + i) * LANES, LANES), LANES)
                A[:, one] = (jax.nn.silu(summed[:, :LANES]) * summed[:, LANES:]).astype(jnp.bfloat16)
                return 0

            lax.fori_loop(0, pairs, tile, 0)

        return run

    pieces, held = [], []
    chip, core, chips = t // 2, lax.rem(t, 2), tp // 2
    half = rows // 2
    mine = pl.ds(pl.multiple_of(core * half, half), half)
    theirs = pl.ds(pl.multiple_of((1 - core) * half, half), half)
    partner = t + 1 - 2 * core

    def launch(when, make):
        @pl.when(when)
        def _():
            make().start()

        pieces.append((when, make))

    def add_up():
        while held:
            index, s, lanes, peer, place = held.pop()
            away = peer // 2 != chip

            def onward():
                return remote(
                    V.at[:, lanes], R2.at[chip, mine, place],
                    r2_send.at[index, s], r2_recv.at[chip, core, place_index(place)], "tp", peer,
                )

            @pl.when(away)
            def _():
                remote(
                    B.at[:, lanes], B.at[:, lanes], b_send.at[index, s], b_recv.at[index, s], "tp", partner
                ).wait_recv()
                V[:, lanes] = (T[mine, lanes].astype(jnp.float32) + B[:, lanes].astype(jnp.float32)).astype(
                    jnp.bfloat16
                )
                onward().start()

            pieces.append((away, onward))

    def place_index(place):
        return place.start // LANES

    def down(index, s):
        first, wide = dn_groups[index]

        def run():
            while mixed:
                mixed.pop().wait_send()
            add_up()
            owner = nearest(s)
            if s:
                settled(tags[("dn", index)], owner)
            start = owner * col + first
            lanes = pl.ds(pl.multiple_of(start, LANES), wide)
            peer = start // dc
            place = pl.ds(pl.multiple_of(start - peer * dc, LANES), wide)
            T[:, lanes] = jnp.dot(A[...], Wd[:, lanes], preferred_element_type=jnp.float32).astype(jnp.bfloat16)
            launch(
                peer == partner,
                lambda: remote(
                    T.at[:, lanes], R2.at[chip, :, place],
                    r2_send.at[index, s], r2_recv.at[chip, 0, place_index(place)], "tp", partner,
                ),
            )
            launch(
                peer // 2 != chip,
                lambda: remote(
                    T.at[theirs, lanes], B.at[:, lanes], b_send.at[index, s], b_recv.at[index, s], "tp", partner
                ),
            )
            held.append((index, s, lanes, peer, place))

        return run

    def finish():
        add_up()
        for part in range(dc // col):
            for first, wide in dn_groups:
                place = pl.ds(part * col + first, wide)
                at = place_index(place)
                whole = R2.at[chip, :, place]
                remote(whole, whole, r2_send.at[0, 0], r2_recv.at[chip, 0, at], "tp", partner).wait_recv()
                for k in range(1, chips):
                    other = lax.rem(chip + k, chips)
                    for h in range(2):
                        piece = R2.at[other, h * half : (h + 1) * half, place]
                        remote(piece, piece, r2_send.at[0, 0], r2_recv.at[other, h, at], "tp", partner).wait_recv()

        writes = []
        for i in range(rows // SEQ_LEN):
            here = slice(i * SEQ_LEN, (i + 1) * SEQ_LEN)
            total = T[here, pl.ds(pl.multiple_of(t * dc, dc), dc)].astype(jnp.float32)
            for k in range(chips):
                total = total + R2[k, here, :].astype(jnp.float32)
            E[here, :] = (H[t, here, :].astype(jnp.float32) + total).astype(jnp.bfloat16)
            writes.append(pltpu.make_async_copy(E.at[here, :], out.at[here, :], out_sem.at[i]))
            writes[-1].start()
        for write in writes:
            write.wait()

    link = 2 * 2 / 91e3
    costs = [chunk[2] * link for chunk in chunks]
    ring, passed = ring_plan(costs, [chunk[3] for chunk in chunks], n, 5.0)
    events = [(when, 0, c, s, None) for when, c, s in ring]

    def ready(tag, s=None):
        return passed[(tags[tag], n - 1 if s is None else s)]

    clock = [0.0]

    def task(when, takes, run):
        clock[0] = max(clock[0], when)
        events.append((clock[0], 1, len(events), 0, run))
        clock[0] += takes

    across = tp * rows * dc * link / 2
    task(3.0, 1.0, send_scales)
    task(20.0, 0.5, scale_sum)
    task(across, 3.0, first_norm)
    spare = 3.0
    task(ready(("in", len(in_cuts) - 1)) + spare, 2.0, project("in", in_cuts, rec))
    task(ready(("gate", len(gate_cuts) - 1)) + spare, 2.0, project("gate", gate_cuts, 0))
    sequences = rows // SEQ_LEN
    for first, many in parted(sequences, 3):
        task(ready("blk"), 6.0 * many / sequences, recurrence(first, many))
    task(ready("out") + spare, 3.0, mix_out)
    task(clock[0] + across, 2.0, hidden)
    task(clock[0] + across, 3.0, second_norm)
    for index, (first, pairs) in enumerate(ff_groups):
        for start in range(0, pairs, 2):
            many = min(2, pairs - start)
            task(ready(("ff", index)) + spare, 1.0 * many, activate(index, first + start, many, start == 0))
    def arrived(index, s):
        if s == 0:
            return 0.0
        whole = ready(("dn", index), s)
        return max(whole, ready("solo", s)) if index == len(dn_groups) - 1 else whole

    last = [(arrived(index, s), index, s) for index in range(len(dn_groups)) for s in range(n)]
    for when, index, s in sorted(last):
        task(when, 1.3, down(index, s))
    for _, kind, c, s, run in sorted(events, key=lambda e: e[:4]):
        if kind == 0:
            line_step(c, s)
        else:
            run()
    finish()
    for copy, when in drains:
        if when is None:
            copy.wait_send()
        else:
            @pl.when(when)
            def _(copy=copy):
                copy.wait_send()

    for when, make in pieces:
        @pl.when(when)
        def _(make=make):
            make().wait_send()


def on_device(
    tokens,
    recurrent_norm_gain,
    channel_norm_gain,
    gate_projection_weight,
    gate_column_scale,
    input_projection_weight,
    input_column_scale,
    convolution_kernel,
    recurrence_gate_weight,
    recurrence_column_scale,
    input_gate_weight,
    input_gate_column_scale,
    channel_decay_param,
    position_decay_shift,
    output_projection_weight,
    output_column_scale,
    mixer_gate_weight,
    mixer_gate_column_scale,
    up_projection_weight,
    up_column_scale,
    down_projection_weight,
    down_column_scale,
):
    n, copies, tp = (lax.axis_size(axis) for axis in ("fs", "grp", "tp"))
    rows, dc = tokens.shape
    model = dc * tp
    krows, rec = gate_projection_weight.shape
    blocks, brows, width = recurrence_gate_weight.shape
    ff = mixer_gate_weight.shape[1]
    hid = -(-ff // LANES) * LANES
    col = output_projection_weight.shape[1]

    weights = (
        input_projection_weight,
        recurrence_gate_weight,
        input_gate_weight,
        gate_projection_weight,
        output_projection_weight,
        mixer_gate_weight,
        up_projection_weight,
        down_projection_weight,
    )

    dims = (n, copies, tp, rows, model, dc, rec, blocks, brows, width, ff, hid, col)
    chunk_count = 3 + len(first_cuts(rec)) + len(shares(rec // LANES, 2)) + len(shares(hid // LANES, 4)) + len(shares(col // LANES, 3))
    here = pl.BlockSpec(memory_space=pltpu.VMEM)
    away = pl.BlockSpec(memory_space=pl.ANY)
    bf = lambda *shape: pltpu.VMEM(shape, jnp.bfloat16)
    dma = lambda *shape: pltpu.SemaphoreType.DMA(shape)
    flops = 2 * rows * (model * (2 * rec + 2 * hid) + rec * 2 * width + rec * model + hid * model)
    return pl.pallas_call(
        lambda *refs: layer_body(dims, *refs),
        out_shape=jax.ShapeDtypeStruct((rows, dc), jnp.bfloat16),
        in_specs=[away] * 9 + [here] * 13,
        out_specs=away,
        scratch_shapes=[
            pltpu.VMEM(gate_projection_weight.shape, jnp.float32),
            pltpu.VMEM(input_projection_weight.shape, jnp.float32),
            pltpu.VMEM(recurrence_gate_weight.shape, jnp.float32),
            pltpu.VMEM(input_gate_weight.shape, jnp.float32),
            pltpu.VMEM(output_projection_weight.shape, jnp.float32),
            pltpu.VMEM(mixer_gate_weight.shape, jnp.float32),
            pltpu.VMEM(up_projection_weight.shape, jnp.float32),
            pltpu.VMEM(down_projection_weight.shape, jnp.float32),
            bf(model, 2 * rec),
            bf(blocks, n * brows, 2 * width),
            bf(rec, model),
            bf(model, 2 * hid),
            bf(hid, model),
            bf(tp, rows, dc),
            bf(tp, rows, dc),
            bf(rows, model),
            bf(rows, 2 * rec),
            bf(rows, rec),
            bf(rows, model),
            bf(tp - 1, rows, dc),
            bf(tp // 2, rows, dc),
            bf(rows, hid),
            pltpu.VMEM((n, 1, 4 * rec + 2 * hid), jnp.float32),
            pltpu.VMEM((1, 4 * rec + 2 * hid), jnp.float32),
            pltpu.VMEM((1, rec), jnp.float32),
            pltpu.VMEM((8, max(rec, hid)), jnp.float32),
            bf(rows // 2, model),
            bf(rows // 2, model),
            bf(rows, dc),
            dma(2, chunk_count, n),
            dma(chunk_count, n),
            dma(chunk_count, n, copies - 1),
            dma(chunk_count, n, copies - 1),
            dma(len(weights)),
            dma(1),
            dma(tp - 1),
            dma(tp - 1),
            dma(tp - 1),
            dma(tp - 1),
            dma(tp - 1),
            dma(tp - 1),
            dma(len(shares(col // LANES, 3)), n),
            dma(tp // 2, 2, dc // LANES),
            dma(n - 1),
            dma(n - 1),
            dma(len(shares(col // LANES, 3)), n),
            dma(len(shares(col // LANES, 3)), n),
            dma(rows // SEQ_LEN),
        ],
        compiler_params=pltpu.CompilerParams(
            collective_id=0, has_side_effects=True, vmem_limit_bytes=67_043_328
        ),
        cost_estimate=pl.CostEstimate(flops=flops, bytes_accessed=8 * rows * model, transcendentals=0),
    )(
        tokens,
        *weights,
        output_column_scale[None, :],
        down_column_scale[None, :],
        gate_column_scale[None, :],
        input_column_scale[None, :],
        recurrence_column_scale,
        input_gate_column_scale,
        mixer_gate_column_scale,
        up_column_scale,
        recurrent_norm_gain[None, :],
        channel_norm_gain[None, :],
        convolution_kernel,
        channel_decay_param[None, :],
        position_decay_shift.reshape(-1, SEQ_LEN),
    )


def solution(mesh):
    placed = (
        P(("grp", "fs"), "tp"),
        P(),
        P(),
        P("fs", "tp"),
        P(("tp", "fs")),
        P("fs", "tp"),
        P(("tp", "fs")),
        P(None, "tp"),
        P("tp", "fs", None),
        P("tp", "fs"),
        P("tp", "fs", None),
        P("tp", "fs"),
        P("tp"),
        P(("grp", "fs")),
        P("tp", "fs"),
        P("fs"),
        P("fs", "tp"),
        P(("tp", "fs")),
        P("fs", "tp"),
        P(("tp", "fs")),
        P("tp", "fs"),
        P("fs"),
    )
    return jax.shard_map(
        on_device, mesh=mesh, in_specs=placed, out_specs=P(("grp", "fs"), "tp"), check_vma=False
    )
```

```python
import jax
import jax.numpy as jnp
from jax import lax
from jax.experimental import pallas as pl
from jax.experimental.pallas import tpu as pltpu
from jax.sharding import PartitionSpec as P

TAPS = 4
SEQ_LEN = 128
LANES = 128
TILE = 64
MESH = pl.DeviceIdType.MESH

eps = 1e-06


def shares(total, parts):
    parts = min(parts, total)
    return [total // parts + (1 if i < total % parts else 0) for i in range(parts)]


def parted(total, parts):
    spans, first = [], 0
    for many in shares(total, parts):
        spans.append((first, many))
        first += many
    return spans


def solo_rows(deep):
    return deep * 3 // 8 // LANES * LANES


def first_cuts(width):
    cuts = []
    for k in (1, 1, 2):
        if sum(cuts) + k * LANES < width:
            cuts.append(k * LANES)
    return cuts + [width - sum(cuts)]


def ring_plan(costs, solo, count, latency):
    ready = {(c, 0): 0.0 for c in range(len(costs))}
    free, plan, landed = 0.0, [], {}
    while ready:
        at_hand = [k for k in ready if ready[k] <= free]
        if not at_hand:
            free = min(ready.values())
            continue
        c, s = min(at_hand, key=lambda k: (k[0], -k[1]))
        begin = free
        del ready[(c, s)]
        free = free + costs[c]
        landed[(c, s)] = free + (2.5 if free < 10.0 else latency)
        plan.append((begin, c, s))
        if s + 1 < count - 1:
            ready[(c, s + 1)] = landed[(c, s)]
    for c in range(len(costs)):
        plan.append((landed[(c, count - 2)], c, count - 1))
    passed, free = {}, 0.0
    for when, c, s in sorted((landed[k], k[0], k[1] + 1) for k in landed):
        if solo[c]:
            passed[(c, s)] = when
        else:
            free = max(free, when) + costs[c]
            passed[(c, s)] = free + latency
    return sorted(plan), passed


def layer_body(dims, *refs):
    (n, copies, tp, rows, model, dc, rec, blocks, brows, width, ff, hid, col) = dims
    tokens, weights, (
        out_scale, down_scale, gate_scale, in_scale, recur_scale, inject_scale, swish_scale, up_scale,
        gain1, gain2, taps, decay_param, shift, out,
        Fg, Fi, Fr, Fj, Fo, Fs, Fu, Fd,
        Wp, Wb, Wo, Wf, Wd, X, H, N, UG, M, T, R1, R2, A, S, SV, SP, Z, B, V, E,
        z_send, z_recv, y_send, y_recv, own_sem, tok_sem,
        x_send, x_recv, r1_send, r1_recv, h_send, h_recv, r2_send, r2_recv, s_send, s_recv,
        b_send, b_recv, out_sem,
    ) = refs[0], refs[1:9], refs[9:]
    g, f, t = lax.axis_index("grp"), lax.axis_index("fs"), lax.axis_index("tp")
    krows = model // n

    barrier = pltpu.get_barrier_semaphore()
    for axis, count, here in (("fs", n, f), ("grp", copies, g), ("tp", tp, t)):
        for k in range(1, count):
            pl.semaphore_signal(
                barrier, inc=1, device_id={axis: lax.rem(here + k, count)}, device_id_type=MESH
            )

    def remote(src, dst, send, recv, axis, index):
        return pltpu.make_async_remote_copy(
            src_ref=src, dst_ref=dst, send_sem=send, recv_sem=recv,
            device_id={axis: index}, device_id_type=MESH,
        )

    staged = (Fi, Fr, Fj, Fg, Fo, Fs, Fu, Fd)
    loads = {}
    for k, (source, place) in sorted(enumerate(zip(weights, staged)), key=lambda e: (e[0] not in (1, 2), e[0])):
        loads[k] = pltpu.make_async_copy(source, place, own_sem.at[k])
        loads[k].start()
    tok = pltpu.make_async_copy(tokens, X.at[t], tok_sem.at[0])
    tok.start()

    def loaded(*which):
        for k in which:
            if k in loads:
                loads.pop(k).wait()

    def by_tiles(total, step, run):
        def tile(i, _):
            run(pl.multiple_of(i * step, step))
            return 0

        lax.fori_loop(0, total // step, tile, 0)

    chunks, tags = [], {}

    def by_rows(buf, first, wide, parts):
        per = krows // copies

        def view(owner, share):
            return buf.at[pl.ds(pl.multiple_of(owner * krows + share * per, per), per), pl.ds(first, wide)]

        def fill():
            loaded(*(k for k, _, _, _ in parts))

            def tile(at):
                here = pl.ds(pl.multiple_of(f * krows + at, TILE), TILE)
                for k, source, start, many in parts:
                    got = staged[k][pl.ds(at, TILE), source : source + many].astype(jnp.bfloat16)
                    buf[here, start : start + many] = got

            by_tiles(krows, TILE, tile)

        return view, fill, per * wide, False

    def by_columns(buf, k, scale, first, wide, top=0, bottom=None, solo=False):
        deep = (buf.shape[0] if bottom is None else bottom) - top
        height = min(deep, staged[k].shape[0] - top)
        per = deep if solo else deep // copies

        def view(owner, share):
            start = top if solo else pl.multiple_of(top + share * per, 16)
            return buf.at[pl.ds(start, per), pl.ds(pl.multiple_of(owner * col + first, LANES), wide)]

        def fill():
            loaded(k)
            lanes = pl.ds(pl.multiple_of(f * col + first, LANES), wide)

            def tile(at):
                here = pl.ds(pl.multiple_of(top + at, TILE), TILE)
                got = staged[k][here, first : first + wide] * scale[:, first : first + wide]
                buf[here, lanes] = got.astype(jnp.bfloat16)

            by_tiles(height, TILE, tile)
            if deep > height:
                buf[top + height : top + deep, lanes] = jnp.zeros((deep - height, wide), jnp.bfloat16)

        return view, fill, per * wide, solo

    def by_blocks():
        per = 2 * width // copies

        def view(owner, share):
            return Wb.at[
                :, pl.ds(pl.multiple_of(owner * brows, brows), brows),
                pl.ds(pl.multiple_of(share * per, per), per),
            ]

        def fill():
            loaded(1, 2)
            here = pl.ds(pl.multiple_of(f * brows, brows), brows)
            Wb[:, here, :width] = Fr[...].astype(jnp.bfloat16)
            Wb[:, here, width:] = Fj[...].astype(jnp.bfloat16)

        return view, fill, blocks * brows * per, False

    def by_pairs(first, pairs):
        parts = []
        for i in range(first, first + pairs):
            many = min(LANES, ff - i * LANES)
            parts.append((5, i * LANES, 2 * i * LANES, many))
            parts.append((6, i * LANES, (2 * i + 1) * LANES, many))
        return by_rows(Wf, first * 2 * LANES, pairs * 2 * LANES, parts)

    if hid > ff:
        own_rows = pl.ds(pl.multiple_of(f * krows, krows), krows)
        Wf[own_rows, 2 * (hid - LANES) : 2 * hid] = jnp.zeros((krows, 2 * LANES), jnp.bfloat16)

    def add(tag, chunk):
        tags[tag] = len(chunks)
        chunks.append(chunk)

    add("blk", by_blocks())
    def add_projection(tag, k, base, cuts):
        start = 0
        for i, wide in enumerate(cuts):
            add((tag, i), by_rows(Wp, base + start, wide, [(k, start, base + start, wide)]))
            start += wide

    in_cuts, gate_cuts = first_cuts(rec), [LANES * k for k in shares(rec // LANES, 2)]
    add_projection("in", 0, rec, in_cuts)
    add_projection("gate", 3, 0, gate_cuts)
    add("out", by_columns(Wo, 4, out_scale, 0, col))
    ff_groups, first = [], 0
    for pairs in shares(hid // LANES, 4):
        add(("ff", len(ff_groups)), by_pairs(first, pairs))
        ff_groups.append((first, pairs))
        first += pairs
    dn_groups, first = [], 0
    for lanes in shares(col // LANES, 3):
        index, at, wide = len(dn_groups), first * LANES, lanes * LANES
        cut = solo_rows(hid) if index == len(shares(col // LANES, 3)) - 1 else 0
        add(("dn", index), by_columns(Wd, 7, down_scale, at, wide, cut, hid))
        if cut:
            add("solo", by_columns(Wd, 7, down_scale, at, wide, 0, cut, True))
        dn_groups.append((first * LANES, lanes * LANES))
        first += lanes

    chunks[0][1]()
    pl.semaphore_wait(barrier, (n - 1) + (copies - 1) + (tp - 1))

    drains = []

    def send(copy, when=None):
        if when is None:
            copy.start()
        else:
            @pl.when(when)
            def _():
                copy.start()

        drains.append((copy, when))

    def z_copy(c, owner, side):
        view = chunks[c][0](owner, g)
        return remote(
            view, view, z_send.at[side, c, owner], z_recv.at[c, owner], "fs",
            jnp.clip(f - 1 if side else f + 1, 0, n - 1),
        )

    def y_copy(c, owner, other, share):
        view = chunks[c][0](owner, share)
        return remote(
            view, view, y_send.at[c, owner, other - 1], y_recv.at[c, owner, other - 1],
            "grp", lax.rem(g + other, copies),
        )

    def passing(c):
        return range(1, 1 if chunks[c][3] else copies)

    def line_step(c, s):
        if s == 0 and c:
            chunks[c][1]()
        for side in range(2):
            owner = jnp.clip(f + s if side else f - s, 0, n - 1)
            here = f + s < n if side else f >= s
            onward = f > 0 if side else f < n - 1
            if s:
                @pl.when(here)
                def _():
                    z_copy(c, owner, side).wait_recv()
                    for other in passing(c):
                        y_copy(c, owner, other, g).start()

                for other in passing(c):
                    drains.append((y_copy(c, owner, other, g), here))
            send(z_copy(c, owner, side), jnp.logical_and(here, onward))

    def settled(c, owner):
        for other in passing(c):
            y_copy(c, owner, other, lax.rem(g - other + copies, copies)).wait_recv()

    def gathered(c):
        for k in range(1, n):
            settled(c, lax.rem(f + k, n))

    def nearest(m):
        near = jnp.minimum(f, n - 1 - f)
        two = (m + 1) // 2
        paired = f - two if m % 2 else f + two
        single = jnp.where(f < n - 1 - f, f + (m - near), f - (m - near))
        return jnp.where(m <= 2 * near, paired, single)

    def spread(source, buf, sends, recvs):
        for k in range(1, tp):
            send(remote(source, buf.at[t], sends.at[k - 1], recvs.at[k - 1], "tp", lax.rem(t + k, tp)))

    def spread_land(buf, sends, recvs):
        for k in range(1, tp):
            place = buf.at[lax.rem(t - k + tp, tp)]
            remote(place, place, sends.at[k - 1], recvs.at[k - 1], "tp", lax.rem(t + k, tp)).wait_recv()

    spread(tokens, X, x_send, x_recv)

    def send_scales():
        def placed(scale, wide):
            many = scale.shape[-1]
            scale = scale.reshape(1, many)
            Z[:, :wide] = jnp.zeros((8, wide), jnp.float32)
            Z[:, :many] = jnp.broadcast_to(scale, (8, many))
            return pltpu.roll(Z[:, :wide], f * many, 1)[0:1]

        S[f, :, 0:rec] = placed(gate_scale[...], rec)
        S[f, :, rec : 2 * rec] = placed(in_scale[...], rec)
        for base, scale in ((2 * rec, recur_scale), (3 * rec, inject_scale)):
            for block in range(blocks):
                at = base + block * width
                S[f, :, at : at + width] = placed(scale[block : block + 1, :], width)
        for half, scale in enumerate((swish_scale, up_scale)):
            whole = placed(scale[...], hid)
            for i in range(hid // LANES):
                at = 4 * rec + (2 * i + half) * LANES
                S[f, :, at : at + LANES] = whole[:, i * LANES : (i + 1) * LANES]
        for k in range(1, n):
            send(remote(S.at[f], S.at[f], s_send.at[k - 1], s_recv.at[k - 1], "fs", lax.rem(f + k, n)))
        lost = -decay_param[...]
        u = jnp.exp(-jnp.abs(lost))
        z = u / (2.0 + u)
        square, tail = z * z, 0.0
        for odd in range(17, 0, -2):
            tail = tail * square + 1.0 / odd
        SP[...] = jnp.maximum(lost, 0.0) + 2.0 * z * tail

    def norm(buf, gain):
        def tile(i, _):
            here = pl.ds(pl.multiple_of(i * SEQ_LEN, SEQ_LEN), SEQ_LEN)
            parts = [buf[p, here, :].astype(jnp.float32) for p in range(tp)]
            total = sum(jnp.sum(v * v, axis=-1, keepdims=True) for v in parts)
            factor = lax.rsqrt(total / model + eps)
            for p in range(tp):
                lanes = slice(p * dc, (p + 1) * dc)
                N[here, lanes] = (parts[p] * factor * gain[:, lanes]).astype(jnp.bfloat16)
            return 0

        lax.fori_loop(0, rows // SEQ_LEN, tile, 0)

    def first_norm():
        tok.wait()
        spread_land(X, x_send, x_recv)
        norm(X, gain1)

    def project(tag, cuts, first):
        def run():
            for i in range(len(cuts)):
                gathered(tags[(tag, i)])

            def tile(i, _):
                lanes = pl.ds(pl.multiple_of(first + i * 256, LANES), 256)
                summed = jnp.dot(N[...], Wp[:, lanes], preferred_element_type=jnp.float32)
                UG[:, lanes] = (summed * SV[:, lanes]).astype(jnp.bfloat16)
                return 0

            lax.fori_loop(0, rec // 256, tile, 0)

        return run

    def scale_sum():
        for k in range(1, n):
            place = S.at[lax.rem(f - k + n, n)]
            remote(place, place, s_send.at[k - 1], s_recv.at[k - 1], "fs", lax.rem(f + k, n)).wait_recv()
        total = S[0]
        for o in range(1, n):
            total = total + S[o]
        SV[...] = total

    def recurrence(first, many):
        return lambda: sequences_of(first, many)

    def sequences_of(first, many):
        if first == 0:
            gathered(tags["blk"])
        position = lax.broadcasted_iota(jnp.int32, (SEQ_LEN, width), 0)
        square = (SEQ_LEN, SEQ_LEN)
        diagonal = lax.broadcasted_iota(jnp.int32, square, 0) == lax.broadcasted_iota(jnp.int32, square, 1)

        def sequence(i, _):
            here = pl.ds(pl.multiple_of(i * SEQ_LEN, SEQ_LEN), SEQ_LEN)
            along = jnp.broadcast_to(shift[pl.ds(i, 1), :], (SEQ_LEN, SEQ_LEN))
            moved_by = jnp.sum(jnp.where(diagonal, along, 0.0), axis=1, keepdims=True)
            for block in range(blocks):
                lanes = slice(block * width, (block + 1) * width)
                at = lambda base: slice(base + block * width, base + (block + 1) * width)
                branch = UG[here, at(rec)].astype(jnp.float32)
                summed = branch * taps[0:1, lanes]
                for offset in range(1, TAPS):
                    moved = jnp.where(position >= offset, pltpu.roll(branch, offset, 0), 0.0)
                    summed = summed + moved * taps[offset : offset + 1, lanes]
                conv = summed.astype(jnp.bfloat16)
                sums = jnp.dot(conv, Wb[block], preferred_element_type=jnp.float32)
                recur = jax.nn.sigmoid(sums[:, :width] * SV[:, at(2 * rec)])
                inject = jax.nn.sigmoid(sums[:, width:] * SV[:, at(3 * rec)])
                log_keep = -8.0 * recur * SP[:, lanes] + moved_by
                twice = 2.0 * log_keep
                near = -twice * (
                    1.0
                    + twice * (0.5 + twice * (1.0 / 6 + twice * (1.0 / 24 + twice * (1.0 / 120))))
                )
                lost = jnp.where(twice > -0.125, near, 1.0 - jnp.exp(twice))
                factor = jnp.where(position == 0, 1.0, jnp.sqrt(lost))
                state = conv.astype(jnp.float32) * inject * factor
                keep = jnp.exp(log_keep)
                reach = 1
                while reach < SEQ_LEN:
                    inside = position >= reach
                    state = state + keep * jnp.where(inside, pltpu.roll(state, reach, 0), 0.0)
                    keep = keep * jnp.where(inside, pltpu.roll(keep, reach, 0), 1.0)
                    reach *= 2
                gate = UG[here, lanes].astype(jnp.float32)
                M[here, lanes] = (jax.nn.gelu(gate) * state).astype(jnp.bfloat16)
            return 0

        lax.fori_loop(first, first + many, sequence, 0)

    mixed = []

    def mix_out():
        gathered(tags["out"])
        for k in list(range(1, tp)) + [0]:
            peer = lax.rem(t + k, tp)
            lanes = pl.ds(pl.multiple_of(peer * dc, dc), dc)
            T[:, lanes] = jnp.dot(M[...], Wo[:, lanes], preferred_element_type=jnp.float32).astype(jnp.bfloat16)
            if k:
                mixed.append(
                    remote(T.at[:, lanes], R1.at[k - 1], r1_send.at[k - 1], r1_recv.at[k - 1], "tp", peer)
                )
                mixed[-1].start()

    def hidden():
        for k in range(1, tp):
            place = R1.at[k - 1]
            remote(place, place, r1_send.at[k - 1], r1_recv.at[k - 1], "tp", lax.rem(t + k, tp)).wait_recv()

        def tile(i, _):
            here = pl.ds(pl.multiple_of(i * SEQ_LEN, SEQ_LEN), SEQ_LEN)
            total = T[here, pl.ds(pl.multiple_of(t * dc, dc), dc)].astype(jnp.float32)
            for k in range(1, tp):
                total = total + R1[k - 1, here, :].astype(jnp.float32)
            H[t, here, :] = (X[t, here, :].astype(jnp.float32) + total).astype(jnp.bfloat16)
            return 0

        lax.fori_loop(0, rows // SEQ_LEN, tile, 0)
        spread(H.at[t], H, h_send, h_recv)

    def second_norm():
        spread_land(H, h_send, h_recv)
        norm(H, gain2)

    def activate(index, first, pairs, opens):
        def run():
            if opens:
                gathered(tags[("ff", index)])

            def tile(i, _):
                both = pl.ds(pl.multiple_of((first + i) * 2 * LANES, 2 * LANES), 2 * LANES)
                cols = pl.ds(pl.multiple_of(4 * rec + (first + i) * 2 * LANES, LANES), 2 * LANES)
                summed = jnp.dot(N[...], Wf[:, both], preferred_element_type=jnp.float32)
                summed = summed * SV[:, cols]
                one = pl.ds(pl.multiple_of((first + i) * LANES, LANES), LANES)
                A[:, one] = (jax.nn.silu(summed[:, :LANES]) * summed[:, LANES:]).astype(jnp.bfloat16)
                return 0

            lax.fori_loop(0, pairs, tile, 0)

        return run

    pieces, held = [], []
    chip, core, chips = t // 2, lax.rem(t, 2), tp // 2
    half = rows // 2
    mine = pl.ds(pl.multiple_of(core * half, half), half)
    theirs = pl.ds(pl.multiple_of((1 - core) * half, half), half)
    partner = t + 1 - 2 * core

    def launch(when, make):
        @pl.when(when)
        def _():
            make().start()

        pieces.append((when, make))

    def add_up():
        while held:
            index, s, lanes, peer, place = held.pop()
            away = peer // 2 != chip

            def onward():
                return remote(
                    V.at[:, lanes], R2.at[chip, mine, place],
                    r2_send.at[index, s], r2_recv.at[chip, core, place_index(place)], "tp", peer,
                )

            @pl.when(away)
            def _():
                remote(
                    B.at[:, lanes], B.at[:, lanes], b_send.at[index, s], b_recv.at[index, s], "tp", partner
                ).wait_recv()
                V[:, lanes] = (T[mine, lanes].astype(jnp.float32) + B[:, lanes].astype(jnp.float32)).astype(
                    jnp.bfloat16
                )
                onward().start()

            pieces.append((away, onward))

    def place_index(place):
        return place.start // LANES

    def down(index, s):
        first, wide = dn_groups[index]

        def run():
            while mixed:
                mixed.pop().wait_send()
            add_up()
            owner = nearest(s)
            if s:
                settled(tags[("dn", index)], owner)
            start = owner * col + first
            lanes = pl.ds(pl.multiple_of(start, LANES), wide)
            peer = start // dc
            place = pl.ds(pl.multiple_of(start - peer * dc, LANES), wide)
            T[:, lanes] = jnp.dot(A[...], Wd[:, lanes], preferred_element_type=jnp.float32).astype(jnp.bfloat16)
            launch(
                peer == partner,
                lambda: remote(
                    T.at[:, lanes], R2.at[chip, :, place],
                    r2_send.at[index, s], r2_recv.at[chip, 0, place_index(place)], "tp", partner,
                ),
            )
            launch(
                peer // 2 != chip,
                lambda: remote(
                    T.at[theirs, lanes], B.at[:, lanes], b_send.at[index, s], b_recv.at[index, s], "tp", partner
                ),
            )
            held.append((index, s, lanes, peer, place))

        return run

    def finish():
        add_up()
        for part in range(dc // col):
            for first, wide in dn_groups:
                place = pl.ds(part * col + first, wide)
                at = place_index(place)
                whole = R2.at[chip, :, place]
                remote(whole, whole, r2_send.at[0, 0], r2_recv.at[chip, 0, at], "tp", partner).wait_recv()
                for k in range(1, chips):
                    other = lax.rem(chip + k, chips)
                    for h in range(2):
                        piece = R2.at[other, h * half : (h + 1) * half, place]
                        remote(piece, piece, r2_send.at[0, 0], r2_recv.at[other, h, at], "tp", partner).wait_recv()

        writes = []
        for i in range(rows // SEQ_LEN):
            here = slice(i * SEQ_LEN, (i + 1) * SEQ_LEN)
            total = T[here, pl.ds(pl.multiple_of(t * dc, dc), dc)].astype(jnp.float32)
            for k in range(chips):
                total = total + R2[k, here, :].astype(jnp.float32)
            E[here, :] = (H[t, here, :].astype(jnp.float32) + total).astype(jnp.bfloat16)
            writes.append(pltpu.make_async_copy(E.at[here, :], out.at[here, :], out_sem.at[i]))
            writes[-1].start()
        for write in writes:
            write.wait()

    link = 2 * 2 / 93.5e3
    costs = [chunk[2] * link for chunk in chunks]
    ring, passed = ring_plan(costs, [chunk[3] for chunk in chunks], n, 4.0)
    events = [(when, 0, c, s, None) for when, c, s in ring]

    def ready(tag, s=None):
        return passed[(tags[tag], n - 1 if s is None else s)]

    clock = [0.0]

    def task(when, takes, run):
        clock[0] = max(clock[0], when)
        events.append((clock[0], 1, len(events), 0, run))
        clock[0] += takes

    across = tp * rows * dc * link / 2
    task(3.0, 1.0, send_scales)
    task(20.0, 0.5, scale_sum)
    task(across, 3.0, first_norm)
    spare = 3.0
    task(ready(("in", len(in_cuts) - 1)) + spare, 2.0, project("in", in_cuts, rec))
    task(ready(("gate", len(gate_cuts) - 1)) + spare, 2.0, project("gate", gate_cuts, 0))
    sequences = rows // SEQ_LEN
    for first, many in parted(sequences, 3):
        task(ready("blk"), 6.0 * many / sequences, recurrence(first, many))
    task(ready("out") + spare, 3.0, mix_out)
    task(clock[0] + across, 2.0, hidden)
    task(clock[0] + across, 3.0, second_norm)
    for index, (first, pairs) in enumerate(ff_groups):
        for start in range(0, pairs, 2):
            many = min(2, pairs - start)
            task(ready(("ff", index)) + spare, 1.0 * many, activate(index, first + start, many, start == 0))
    def arrived(index, s):
        if s == 0:
            return 0.0
        whole = ready(("dn", index), s)
        return max(whole, ready("solo", s)) if index == len(dn_groups) - 1 else whole

    last = [(arrived(index, s), index, s) for index in range(len(dn_groups)) for s in range(n)]
    for when, index, s in sorted(last):
        task(when, 1.3, down(index, s))
    for _, kind, c, s, run in sorted(events, key=lambda e: e[:4]):
        if kind == 0:
            line_step(c, s)
        else:
            run()
    finish()
    for copy, when in drains:
        if when is None:
            copy.wait_send()
        else:
            @pl.when(when)
            def _(copy=copy):
                copy.wait_send()

    for when, make in pieces:
        @pl.when(when)
        def _(make=make):
            make().wait_send()


def on_device(
    tokens,
    recurrent_norm_gain,
    channel_norm_gain,
    gate_projection_weight,
    gate_column_scale,
    input_projection_weight,
    input_column_scale,
    convolution_kernel,
    recurrence_gate_weight,
    recurrence_column_scale,
    input_gate_weight,
    input_gate_column_scale,
    channel_decay_param,
    position_decay_shift,
    output_projection_weight,
    output_column_scale,
    mixer_gate_weight,
    mixer_gate_column_scale,
    up_projection_weight,
    up_column_scale,
    down_projection_weight,
    down_column_scale,
):
    n, copies, tp = (lax.axis_size(axis) for axis in ("fs", "grp", "tp"))
    rows, dc = tokens.shape
    model = dc * tp
    krows, rec = gate_projection_weight.shape
    blocks, brows, width = recurrence_gate_weight.shape
    ff = mixer_gate_weight.shape[1]
    hid = -(-ff // LANES) * LANES
    col = output_projection_weight.shape[1]

    weights = (
        input_projection_weight,
        recurrence_gate_weight,
        input_gate_weight,
        gate_projection_weight,
        output_projection_weight,
        mixer_gate_weight,
        up_projection_weight,
        down_projection_weight,
    )

    dims = (n, copies, tp, rows, model, dc, rec, blocks, brows, width, ff, hid, col)
    chunk_count = 3 + len(first_cuts(rec)) + len(shares(rec // LANES, 2)) + len(shares(hid // LANES, 4)) + len(shares(col // LANES, 3))
    here = pl.BlockSpec(memory_space=pltpu.VMEM)
    away = pl.BlockSpec(memory_space=pl.ANY)
    bf = lambda *shape: pltpu.VMEM(shape, jnp.bfloat16)
    dma = lambda *shape: pltpu.SemaphoreType.DMA(shape)
    flops = 2 * rows * (model * (2 * rec + 2 * hid) + rec * 2 * width + rec * model + hid * model)
    return pl.pallas_call(
        lambda *refs: layer_body(dims, *refs),
        out_shape=jax.ShapeDtypeStruct((rows, dc), jnp.bfloat16),
        in_specs=[away] * 9 + [here] * 13,
        out_specs=away,
        scratch_shapes=[
            pltpu.VMEM(gate_projection_weight.shape, jnp.float32),
            pltpu.VMEM(input_projection_weight.shape, jnp.float32),
            pltpu.VMEM(recurrence_gate_weight.shape, jnp.float32),
            pltpu.VMEM(input_gate_weight.shape, jnp.float32),
            pltpu.VMEM(output_projection_weight.shape, jnp.float32),
            pltpu.VMEM(mixer_gate_weight.shape, jnp.float32),
            pltpu.VMEM(up_projection_weight.shape, jnp.float32),
            pltpu.VMEM(down_projection_weight.shape, jnp.float32),
            bf(model, 2 * rec),
            bf(blocks, n * brows, 2 * width),
            bf(rec, model),
            bf(model, 2 * hid),
            bf(hid, model),
            bf(tp, rows, dc),
            bf(tp, rows, dc),
            bf(rows, model),
            bf(rows, 2 * rec),
            bf(rows, rec),
            bf(rows, model),
            bf(tp - 1, rows, dc),
            bf(tp // 2, rows, dc),
            bf(rows, hid),
            pltpu.VMEM((n, 1, 4 * rec + 2 * hid), jnp.float32),
            pltpu.VMEM((1, 4 * rec + 2 * hid), jnp.float32),
            pltpu.VMEM((1, rec), jnp.float32),
            pltpu.VMEM((8, max(rec, hid)), jnp.float32),
            bf(rows // 2, model),
            bf(rows // 2, model),
            bf(rows, dc),
            dma(2, chunk_count, n),
            dma(chunk_count, n),
            dma(chunk_count, n, copies - 1),
            dma(chunk_count, n, copies - 1),
            dma(len(weights)),
            dma(1),
            dma(tp - 1),
            dma(tp - 1),
            dma(tp - 1),
            dma(tp - 1),
            dma(tp - 1),
            dma(tp - 1),
            dma(len(shares(col // LANES, 3)), n),
            dma(tp // 2, 2, dc // LANES),
            dma(n - 1),
            dma(n - 1),
            dma(len(shares(col // LANES, 3)), n),
            dma(len(shares(col // LANES, 3)), n),
            dma(rows // SEQ_LEN),
        ],
        compiler_params=pltpu.CompilerParams(
            collective_id=0, has_side_effects=True, vmem_limit_bytes=67_043_328
        ),
        cost_estimate=pl.CostEstimate(flops=flops, bytes_accessed=8 * rows * model, transcendentals=0),
    )(
        tokens,
        *weights,
        output_column_scale[None, :],
        down_column_scale[None, :],
        gate_column_scale[None, :],
        input_column_scale[None, :],
        recurrence_column_scale,
        input_gate_column_scale,
        mixer_gate_column_scale,
        up_column_scale,
        recurrent_norm_gain[None, :],
        channel_norm_gain[None, :],
        convolution_kernel,
        channel_decay_param[None, :],
        position_decay_shift.reshape(-1, SEQ_LEN),
    )


def solution(mesh):
    placed = (
        P(("grp", "fs"), "tp"),
        P(),
        P(),
        P("fs", "tp"),
        P(("tp", "fs")),
        P("fs", "tp"),
        P(("tp", "fs")),
        P(None, "tp"),
        P("tp", "fs", None),
        P("tp", "fs"),
        P("tp", "fs", None),
        P("tp", "fs"),
        P("tp"),
        P(("grp", "fs")),
        P("tp", "fs"),
        P("fs"),
        P("fs", "tp"),
        P(("tp", "fs")),
        P("fs", "tp"),
        P(("tp", "fs")),
        P("tp", "fs"),
        P("fs"),
    )
    return jax.shard_map(
        on_device, mesh=mesh, in_specs=placed, out_specs=P(("grp", "fs"), "tp"), check_vma=False
    )
```
